32 devices in a mesh: grp: 2 (over y), sp: 4 (over z), fs: 2 (over x), tp: 2 (over core).
Axes of the slice: x: 2, y: 2, z: 4, core: 2. Of those that a mesh axis runs over, the one named last changes fastest.
Arguments:
- tokens: bfloat16 [2, 6144, 2048], P('fs', ('grp', 'sp'), 'tp'), parts along dimension 1, may hold values from -12 to 12
- norm_gain: float32 [2048], replicated, may hold values from 0.1 to 1.9
- query_weight: bfloat16 [2048, 16, 64], P(None, 'tp'), may hold values from -3 to 3
- key_weight: bfloat16 [2048, 4, 64], P(None, 'tp'), may hold values from -3 to 3
- value_weight: bfloat16 [2048, 4, 64], P(None, 'tp'), may hold values from -0.125 to 0.125
- sink_logit: float32 [16], P('tp'), may hold values from 1 to 6
- pool_weight: bfloat16 [2048, 4, 256], P(None, None, 'tp'), may hold values from -0.125 to 0.125
- attn_out_weight: bfloat16 [16, 64, 2048], P('tp'), may hold values from -0.5 to 0.5
- pool_out_weight: bfloat16 [4, 256, 2048], P(None, 'tp'), may hold values from -0.1875 to 0.1875
Outputs:
- mixed: bfloat16 [2, 6144, 2048], P('fs', ('grp', 'sp', 'tp')), parts along dimension 1
The draws below stay inside these ranges and needn't reach their ends.
There are 2 independent parts, one for each index of `grp`. The reference program is written for one: setup_inputs(seed, part) draws one part's arguments, and reference() takes and returns one part's arrays. A program takes and returns all parts, laid end to end along the dimension named above; an argument that names none is the same for every part. Nothing has to cross between parts.
All inputs are finite; a program needn't handle non-finite values.
Results may differ from the reference program's by a relative error of at most 0.0095.
The reference program's roundings to bfloat16 on the way (of `normed`, `weight`, `attended` and `pooled`) count: a program that leaves them out, or rounds other values in their place, can miss the bound.
Values may be sent and summed in bfloat16 or wider, within the bound.
A program may use at most 128 MiB of HBM per device.

```python
import jax
import jax.numpy as jnp
from jax import lax

D = 2048
HEADS = 16
KV_HEADS = 4
HEAD_DIM = 64
POOL_CH = 256
WINDOW = 128
TOK_DEV = 768
SEQS = 2
LEN = 3072


def draw_tokens(key, part):
    first, second, third = jax.random.split(jax.random.fold_in(key, 11), 3)
    blocks = LEN // TOK_DEV
    base = jax.random.normal(first, (SEQS, blocks, TOK_DEV, D), jnp.float32)
    offset = jax.random.normal(second, (SEQS, 1, 1, D), jnp.float32)
    factor = jax.random.uniform(third, (SEQS, blocks, 1, 1), jnp.float32, -1.5, 1.5)
    values = jnp.clip(base + factor * offset, -12.0, 12.0)
    return values.reshape(SEQS, LEN, D).astype(jnp.bfloat16)


def projection(key, heads):
    values = jax.random.normal(key, (D, heads, HEAD_DIM), jnp.float32) * D ** (-0.5)
    return jnp.clip(values, -3.0, 3.0).astype(jnp.bfloat16)


def draw_query_weight(key, part):
    return projection(jax.random.fold_in(key, 21), HEADS)


def draw_key_weight(key, part):
    return projection(jax.random.fold_in(key, 31), KV_HEADS)


def block_levels(stream_key, extent, shards, low, top_value):
    def one(dim, blocks):
        heights = jax.random.uniform(jax.random.fold_in(jax.random.fold_in(stream_key, 6), dim), (blocks,), jnp.float32, low / len(shards), top_value / len(shards))
        return jnp.repeat(jnp.exp(heights), extent[dim] // blocks).reshape((-1,) + (1,) * (len(extent) - dim - 1))

    level = one(*shards[0])
    for cut in shards[1:]:
        level = level * one(*cut)
    return level


def noise(own_key, extent, deviation, limit, cuts=(), kind=jnp.bfloat16):
    loudness = block_levels(own_key, extent, cuts, -0.22, 0.18) if cuts else 1.0
    values = jax.random.normal(own_key, extent, jnp.float32) * deviation * loudness
    return jnp.minimum(jnp.maximum(values, -limit), limit).astype(kind)


def setup_inputs(seed: int = 0, part: int = 0) -> dict:
    streams_of = jax.random.split(jax.random.key(seed), 10)
    part_splits = jax.random.split(jax.random.fold_in(streams_of[9], part), 10)
    tokens = draw_tokens(jax.random.fold_in(jax.random.fold_in(streams_of[9], part), 71), part)
    norm_gain = jnp.clip(1.0 + 0.18 * jax.random.normal(streams_of[1], (D,), jnp.float32), 0.1, 1.9)
    query_weight = draw_query_weight(jax.random.fold_in(streams_of[9], 71), part)
    key_weight = draw_key_weight(jax.random.fold_in(streams_of[9], 71), part)
    value_weight = noise(streams_of[4], (D, KV_HEADS, HEAD_DIM), D ** -0.5, 0.125, ((1, 2),))
    sink_logit = jnp.clip(1.0 + 5.0 * jax.random.uniform(streams_of[5], (HEADS,), jnp.float32) ** block_levels(streams_of[5], (HEADS,), ((0, 2),), -0.2, 0.2), 1.0, 6.0)
    pool_weight = noise(streams_of[6], (D, 4, POOL_CH), D ** -0.5, 0.125, ((2, 2),))
    attn_out_weight = noise(streams_of[7], (HEADS, HEAD_DIM, D), (HEADS * HEAD_DIM // 8) ** -0.5, 0.5, ((0, 2),))
    pool_out_weight = noise(streams_of[8], (4, POOL_CH, D), (4 * POOL_CH) ** -0.5, 0.1875, ((1, 2),))
    return dict(tokens=tokens, norm_gain=norm_gain, query_weight=query_weight, key_weight=key_weight, value_weight=value_weight, sink_logit=sink_logit, pool_weight=pool_weight, attn_out_weight=attn_out_weight, pool_out_weight=pool_out_weight)


def rms_norm(rows, gain):
    values = rows.astype(jnp.float32)
    scale = lax.rsqrt(lax.optimization_barrier(jnp.mean(values * values, axis=-1, keepdims=True)) + 1e-06)
    return (values * scale * gain).astype(jnp.bfloat16)

def attend(query, key, value, sinks):
    group = HEADS // KV_HEADS
    blocks = LEN // WINDOW
    qb = query.reshape(blocks, WINDOW, KV_HEADS, group, HEAD_DIM).astype(jnp.float32)

    def banded(tensor):
        tb = tensor.reshape(blocks, WINDOW, KV_HEADS, HEAD_DIM)
        before = jnp.concatenate([jnp.zeros_like(tb[:1]), tb[:-1]], axis=0)
        return jnp.concatenate([before, tb], axis=1).astype(jnp.float32)
    kw = banded(key)
    vw = banded(value)
    qi = jnp.arange(WINDOW, dtype=jnp.int32)[:, None]
    kj = jnp.arange(2 * WINDOW, dtype=jnp.int32)[None, :]
    dist = WINDOW + qi - kj
    inside = (dist >= 0) & (dist < WINDOW)
    key_pos = jnp.arange(blocks, dtype=jnp.int32)[:, None, None] * WINDOW - WINDOW + kj[None]
    mask = inside[None] & (key_pos >= 0)
    scores = jnp.einsum('nqhgd,nkhd->nhgqk', qb, kw) * HEAD_DIM ** (-0.5)
    scores = jnp.where(mask[:, None, None], scores, -jnp.inf)
    sink = sinks.reshape(1, KV_HEADS, group, 1, 1)
    top = jnp.maximum(lax.optimization_barrier(jnp.max(scores, axis=-1, keepdims=True)), sink)
    expo = jnp.exp(scores - top)
    total = lax.optimization_barrier(jnp.sum(expo, axis=-1, keepdims=True)) + jnp.exp(sink - top)
    weight = (expo / total).astype(jnp.bfloat16)
    out = jnp.einsum('nhgqk,nkhd->nqhgd', weight.astype(jnp.float32), vw)
    return out.reshape(LEN, HEADS * HEAD_DIM).astype(jnp.bfloat16)

def pool(pooled_in):
    values = pooled_in.astype(jnp.float32)
    sums = jnp.cumsum(values, axis=0)
    count = jnp.arange(1, LEN + 1).astype(jnp.float32)[:, None]
    parts = []
    for group, reach in enumerate((2, 4, 16)):
        col = sums[:, group]
        lower = jnp.concatenate([jnp.zeros((reach, POOL_CH), jnp.float32), col[:-reach]], axis=0)
        parts.append((col - lower) / jnp.minimum(count, float(reach)))
    parts.append(sums[:, 3] / count)
    mean = jnp.stack(parts, axis=1)
    return (mean - values).astype(jnp.bfloat16)

def one_sequence(rows, norm_gain, query_weight, key_weight, value_weight, sink_logit, pool_weight, attn_out_weight, pool_out_weight):
    normed = rms_norm(rows, norm_gain)
    query = jnp.dot(normed, query_weight.reshape(D, -1), preferred_element_type=jnp.float32).astype(jnp.bfloat16)
    key = jnp.dot(normed, key_weight.reshape(D, -1), preferred_element_type=jnp.float32).astype(jnp.bfloat16)
    value = jnp.dot(normed, value_weight.reshape(D, -1), preferred_element_type=jnp.float32).astype(jnp.bfloat16)
    pooled_in = jnp.dot(normed, pool_weight.reshape(D, -1), preferred_element_type=jnp.float32).astype(jnp.bfloat16)
    attended = attend(query, key, value, sink_logit)
    pooled = pool(pooled_in.reshape(LEN, 4, POOL_CH)).reshape(LEN, 4 * POOL_CH)
    total = jnp.dot(attended, attn_out_weight.reshape(-1, D), preferred_element_type=jnp.float32)
    total = total + jnp.dot(pooled, pool_out_weight.reshape(-1, D), preferred_element_type=jnp.float32)
    return total.astype(jnp.bfloat16)

def reference(tokens, norm_gain, query_weight, key_weight, value_weight, sink_logit, pool_weight, attn_out_weight, pool_out_weight):

    def apply(rows):
        return one_sequence(rows, norm_gain, query_weight, key_weight, value_weight, sink_logit, pool_weight, attn_out_weight, pool_out_weight)
    return lax.map(apply, tokens)
```

```python
import functools

import jax
import jax.numpy as jnp
from jax import lax
from jax.experimental import pallas as pl
from jax.experimental.pallas import tpu as pltpu
from jax.sharding import PartitionSpec as P

MESH = pl.DeviceIdType.MESH
WINDOW = 128
REACHES = (2, 4, 16)
TAIL = 16
CHUNK = 256
COLS = 512
PAIR = 2
F32 = jnp.float32
BF16 = jnp.bfloat16


def dot(a, b, dims=((1,), (0,))):
    return lax.dot_general(a, b, (dims, ((), ())), preferred_element_type=F32)


def kernel(
    n_sp,
    heads,
    local_kv,
    head_dim,
    tokens,
    gain_hbm,
    wq,
    wk,
    wv,
    sink_hbm,
    wp,
    wo,
    wpo,
    out,
    gain,
    sink,
    tri,
    tok,
    normed,
    wqkv,
    wp_raw,
    wp_f32,
    wpool,
    wout,
    qt,
    keys,
    vals,
    ext,
    bands,
    block_sum,
    totals,
    act,
    sending,
    landing,
    w_sem,
    tok_sem,
    tok_send,
    tok_recv,
    halo_send,
    halo_recv,
    tot_send,
    tot_recv,
    out_send,
    out_recv,
    entered,
):
    me_sp = lax.axis_index("sp")
    me_tp = lax.axis_index("tp")
    other = 1 - me_tp
    rows, half_width = tokens.shape
    width = 2 * half_width
    q_rows = heads * head_dim
    kv_rows = local_kv * head_dim
    pool_cols = wpool.shape[1]
    channels = pool_cols // 4
    blocks = rows // WINDOW
    chunks = rows // CHUNK
    per_chunk = CHUNK // WINDOW
    half_rows = rows // 2
    half_blocks = blocks // 2
    tiles = width // COLS
    group = heads // local_kv

    for index in range(n_sp):
        totals[index] = jnp.zeros((8, channels), F32)
    barrier = pltpu.get_barrier_semaphore()
    pl.semaphore_signal(barrier, inc=1, device_id={"tp": other}, device_id_type=MESH)

    @pl.when(me_sp > 0)
    def _():
        pl.semaphore_signal(barrier, inc=1, device_id={"sp": me_sp - 1}, device_id_type=MESH)

    @pl.when(me_sp < n_sp - 1)
    def _():
        pl.semaphore_signal(barrier, inc=1, device_id={"sp": me_sp + 1}, device_id_type=MESH)

    load_wp = pltpu.make_async_copy(wp, wp_raw, w_sem.at[0])

    def local_tokens(c):
        at = pl.ds(pl.multiple_of(c * CHUNK, CHUNK), CHUNK)
        return pltpu.make_async_copy(tokens.at[at, :], tok.at[me_tp, at, :], tok_sem.at[c])

    def remote_tokens(c):
        at = pl.ds(pl.multiple_of(c * CHUNK, CHUNK), CHUNK)
        return pltpu.make_async_remote_copy(
            src_ref=tok.at[me_tp, at, :],
            dst_ref=tok.at[me_tp, at, :],
            send_sem=tok_send.at[c],
            recv_sem=tok_recv.at[c],
            device_id={"tp": other},
            device_id_type=MESH,
        )

    load_gain = pltpu.make_async_copy(gain_hbm, gain, w_sem.at[6])
    load_sink = pltpu.make_async_copy(sink_hbm, sink, w_sem.at[7])
    local_tokens(chunks - 1).start()
    load_wp.start()
    for c in reversed(range(chunks - 1)):
        local_tokens(c).start()
    load_gain.start()
    load_sink.start()
    loads = [
        pltpu.make_async_copy(wq, wqkv.at[pl.ds(0, q_rows), :], w_sem.at[1]),
        pltpu.make_async_copy(wk, wqkv.at[pl.ds(q_rows, kv_rows), :], w_sem.at[2]),
        pltpu.make_async_copy(wv, wqkv.at[pl.ds(q_rows + kv_rows, kv_rows), :], w_sem.at[3]),
    ]
    load_out = [
        pltpu.make_async_copy(wo, wout.at[pl.ds(0, q_rows), :], w_sem.at[4]),
        pltpu.make_async_copy(wpo, wout.at[pl.ds(q_rows, pool_cols), :], w_sem.at[5]),
    ]
    for load in loads:
        load.start()

    target = lax.broadcasted_iota(jnp.int32, (WINDOW, 2 * WINDOW), 0) + WINDOW
    source = lax.broadcasted_iota(jnp.int32, (WINDOW, 2 * WINDOW), 1)
    gap = target - source
    for g, reach in enumerate(REACHES):
        bands[g] = jnp.where((gap >= 0) & (gap < reach), 1.0, 0.0).astype(BF16)
    tri[...] = jnp.where(
        lax.broadcasted_iota(jnp.int32, (WINDOW, PAIR * WINDOW), 0)
        <= lax.rem(lax.broadcasted_iota(jnp.int32, (WINDOW, PAIR * WINDOW), 1), jnp.int32(WINDOW)),
        1.0,
        0.0,
    ).astype(BF16)
    bands[3] = jnp.where((gap >= 0) & (gap < WINDOW) & (source >= WINDOW), 1.0, 0.0).astype(BF16)
    ext[pl.ds(0, WINDOW - TAIL), :] = jnp.zeros((WINDOW - TAIL, pool_cols), BF16)

    @pl.when(me_sp == 0)
    def _():
        ext[pl.ds(WINDOW - TAIL, TAIL), :] = jnp.zeros((TAIL, pool_cols), BF16)
        keys[0] = jnp.zeros((WINDOW, kv_rows), BF16)
        vals[0] = jnp.zeros((kv_rows, WINDOW), BF16)

    neighbours = jnp.where(me_sp > 0, 1, 0) + jnp.where(me_sp < n_sp - 1, 1, 0)
    with jax.named_scope("barrier"):
        pl.semaphore_wait(barrier, 1 + neighbours)
    with jax.named_scope("send_tokens"):
        for c in reversed(range(chunks)):
            local_tokens(c).wait()
            remote_tokens(c).start()
        for load in load_out:
            load.start()

    with jax.named_scope("wait_wp"):
        load_wp.wait()
    part = wp_f32.shape[0]

    def regroup(i, carry):
        wp_f32[...] = wp_raw[pl.ds(pl.multiple_of(i * part, part), part), :].astype(F32)
        at = pl.ds(pl.multiple_of(i * (part // 4), part // 4), part // 4)
        for g in range(4):
            wpool[at, pl.ds(g * channels, channels)] = wp_f32[
                pl.ds(g, part // 4, stride=4), :
            ].astype(BF16)
        return carry

    with jax.named_scope("regroup"):
        lax.fori_loop(0, wp_raw.shape[0] // part, regroup, 0)
    with jax.named_scope("wait_wqkv"):
        for load in loads:
            load.wait()
        load_gain.wait()
        load_sink.wait()

    def halo_copy(buffer, index):
        return pltpu.make_async_remote_copy(
            src_ref=buffer.at[blocks],
            dst_ref=buffer.at[0],
            send_sem=halo_send.at[index],
            recv_sem=halo_recv.at[index],
            device_id={"sp": lax.rem(me_sp + 1, n_sp)},
            device_id_type=MESH,
        )

    halo_keys = halo_copy(keys, 0)
    halo_vals = halo_copy(vals, 2)
    halo_pool = pltpu.make_async_remote_copy(
        src_ref=ext.at[pl.ds(WINDOW + rows - TAIL, TAIL), :],
        dst_ref=ext.at[pl.ds(WINDOW - TAIL, TAIL), :],
        send_sem=halo_send.at[1],
        recv_sem=halo_recv.at[1],
        device_id={"sp": lax.rem(me_sp + 1, n_sp)},
        device_id_type=MESH,
    )

    scale = head_dim ** (-0.5)

    def normalize(c):
        with jax.named_scope("wait_tokens"):
            remote_tokens(c).wait_recv()
        at = pl.ds(pl.multiple_of(c * CHUNK, CHUNK), CHUNK)
        low = tok[0, at, :].astype(F32)
        high = tok[1, at, :].astype(F32)
        square = jnp.sum(low * low, axis=1, keepdims=True)
        square = square + jnp.sum(high * high, axis=1, keepdims=True)
        inv = lax.rsqrt(square * (1.0 / width) + 1e-06)
        normed[c, :, pl.ds(0, half_width)] = (low * inv * gain[:, pl.ds(0, half_width)]).astype(
            BF16
        )
        normed[c, :, pl.ds(half_width, half_width)] = (
            high * inv * gain[:, pl.ds(half_width, half_width)]
        ).astype(BF16)

    def project_pool(c):
        pooled_in = dot(normed[c], wpool[...]).astype(BF16)
        ext[pl.ds(pl.multiple_of(WINDOW + c * CHUNK, WINDOW), CHUNK), :] = pooled_in
        last = pooled_in[:, 3 * channels :].astype(F32)
        for j in range(per_chunk):
            summed = jnp.sum(last[j * WINDOW : (j + 1) * WINDOW], axis=0, keepdims=True)
            block_sum[c * per_chunk + j] = jnp.broadcast_to(summed, (8, channels))

    def project_qkv(c):
        qkv = dot(wqkv[...], normed[c], ((1,), (1,)))
        for j in range(per_chunk):
            b = c * per_chunk + j
            piece = qkv[:, j * WINDOW : (j + 1) * WINDOW]
            qt[b] = (piece[:q_rows] * scale).astype(BF16)
            keys[b + 1] = piece[q_rows : q_rows + kv_rows].T.astype(BF16)
            vals[b + 1] = piece[q_rows + kv_rows :].astype(BF16)

    def hear(step):
        @pl.when(me_sp + step < n_sp - 1)
        def _():
            pl.semaphore_wait(entered.at[step], 1)

    def tell(step):
        @pl.when((me_sp > 0) & (me_sp + step - 1 < n_sp - 1))
        def _():
            pl.semaphore_signal(
                entered.at[step], inc=1, device_id={"sp": me_sp - 1}, device_id_type=MESH
            )

    if n_sp > 2:
        tell(1)

    def project(i, carry):
        c = chunks - 1 - i
        with jax.named_scope("normalize"):
            normalize(c)

        @pl.when((i == 1) & (me_sp < n_sp - 1))
        def _():
            halo_keys.start()
            halo_vals.start()
            halo_pool.start()

        @pl.when(i > 0)
        def _():
            hear(i)
            tell(i + 1)

        with jax.named_scope("project"):
            project_pool(c)
            project_qkv(c)
        return carry

    lax.fori_loop(0, chunks, project, 0)

    for step in range(chunks, n_sp - 1):
        hear(step)
        if step < n_sp - 2:
            tell(step + 1)

    all_rows = block_sum[0]
    for b in range(1, blocks):
        all_rows = all_rows + block_sum[b]
    totals[me_sp] = all_rows

    def total_copy(step):
        return pltpu.make_async_remote_copy(
            src_ref=totals.at[me_sp],
            dst_ref=totals.at[me_sp],
            send_sem=tot_send.at[step],
            recv_sem=tot_recv.at[step],
            device_id={"sp": lax.rem(me_sp + step, n_sp)},
            device_id_type=MESH,
        )

    for step in range(1, n_sp):

        @pl.when(me_sp + step < n_sp)
        def _():
            total_copy(step).start()

    own_key = lax.broadcasted_iota(jnp.int32, (WINDOW, PAIR * WINDOW), 0) <= lax.rem(
        lax.broadcasted_iota(jnp.int32, (WINDOW, PAIR * WINDOW), 1), jnp.int32(WINDOW)
    )
    none = jnp.zeros((head_dim, PAIR * WINDOW), BF16)

    def unit_scores(unit):
        b, slot, h, p, edge = unit
        first_head = h * group + p * PAIR
        q = jnp.concatenate(
            [
                qt[b, pl.ds((first_head + g) * head_dim, head_dim), :]
                for g in range(PAIR)
            ],
            axis=1,
        )
        rhs = jnp.concatenate([q if k == h else none for k in range(local_kv)], axis=0)
        before = dot(keys[b], rhs)
        own = dot(keys[b + 1], rhs)
        return before, own

    def unit_weights(unit, scores):
        b, slot, h, p, edge = unit
        first_head = h * group + p * PAIR
        before, own = scores
        if edge:
            before = before + jnp.where((b == 0) & (me_sp == 0), -jnp.inf, 0.0).astype(F32)
        s = jnp.concatenate(
            [jnp.full((1, WINDOW), sink[first_head + g], F32) for g in range(PAIR)], axis=1
        )
        score = jnp.where(own_key, own, before)
        top = jnp.maximum(jnp.max(score, axis=0, keepdims=True), s)
        expo = jnp.exp(score - top)
        total = jnp.sum(expo, axis=0, keepdims=True) + jnp.exp(s - top)
        weight = (expo * (1.0 / total)).astype(BF16)
        w_own = weight * tri[...]
        return jnp.concatenate([weight - w_own, w_own], axis=0)

    def unit_output(unit, weights):
        b, slot, h, p, edge = unit
        first_head = h * group + p * PAIR
        v_at = pl.ds(h * head_dim, head_dim)
        v = jnp.concatenate([vals[b, v_at, :], vals[b + 1, v_at, :]], axis=1)
        gathered = dot(v, weights)
        stacked = jnp.concatenate(
            [gathered[:, g * WINDOW : (g + 1) * WINDOW] for g in range(PAIR)], axis=0
        )
        act[pl.ds(slot * WINDOW, WINDOW), pl.ds(first_head * head_dim, PAIR * head_dim)] = (
            stacked.T.astype(BF16)
        )

    def attend(units, fillers=()):
        scores, weights = {}, {}
        for step in range(len(units) + 2):
            if step < len(units):
                scores[step] = unit_scores(units[step])
            if step < len(fillers):
                fillers[step]()
            if 0 <= step - 1 < len(units):
                weights[step - 1] = unit_weights(units[step - 1], scores.pop(step - 1))
            if 0 <= step - 2:
                unit_output(units[step - 2], weights.pop(step - 2))

    def units_of(first):
        return [
            (first + i, i, h, p, i == 0)
            for i in range(half_blocks)
            for h in range(local_kv)
            for p in range(group // PAIR)
        ]

    def pool(b, slot, carried):
        start = pl.multiple_of(b * WINDOW, WINDOW)
        position = me_sp * rows + b * WINDOW + 1
        count = (lax.broadcasted_iota(jnp.int32, (WINDOW, channels), 0) + position).astype(F32)
        at = pl.ds(pl.multiple_of(slot * WINDOW, WINDOW), WINDOW)
        for g in range(4):
            col = pl.ds(g * channels, channels)
            own = ext[pl.ds(start + WINDOW, WINDOW), col]
            if g < 3:
                sums = dot(bands[g], ext[pl.ds(start, 2 * WINDOW), col])
                denom = jnp.minimum(count, float(REACHES[g]))
            else:
                base = carried
                for earlier in range(blocks):
                    base = base + jnp.where(earlier < b, block_sum[earlier], 0.0)
                sums = dot(bands[3, :, pl.ds(WINDOW, WINDOW)], own) + base[:1]
                denom = count
            pooled = sums * (1.0 / denom) - own.astype(F32)
            act[at, pl.ds(q_rows + g * channels, channels)] = pooled.astype(BF16)

    with jax.named_scope("wait_halo"):
        @pl.when(me_sp > 0)
        def _():
            halo_keys.wait_recv()
            halo_vals.wait_recv()
            halo_pool.wait_recv()

    def pool_half(first, carried):
        def one(i, carry):
            pool(first + i, i, carried)
            return carry

        lax.fori_loop(0, half_blocks, one, 0, unroll=True)

    first = other * half_blocks
    with jax.named_scope("attend1"):
        attend(units_of(first))
    with jax.named_scope("wait_totals"):
        for step in range(1, n_sp):

            @pl.when(me_sp - step >= 0)
            def _():
                total_copy(step).wait_recv()

    carried = jnp.zeros((8, channels), F32)
    for index in range(n_sp):
        carried = carried + jnp.where(index < me_sp, totals[index], 0.0)
    with jax.named_scope("pool1"):
        pool_half(first, carried)
    for load in load_out:
        load.wait()

    def partial_send(t):
        return pltpu.make_async_remote_copy(
            src_ref=sending.at[t],
            dst_ref=landing.at[t],
            send_sem=out_send.at[t],
            recv_sem=out_recv.at[t],
            device_id={"tp": other},
            device_id_type=MESH,
        )

    def columns(t):
        return pl.ds(pl.multiple_of(t * COLS, COLS), COLS)

    def give(t):
        sending[t] = dot(act[...], wout[:, columns(t)]).astype(BF16)

    with jax.named_scope("give"):
        for t in range(0, tiles, 2):
            give(t)
            give(t + 1)
            partial_send(t).start()
            partial_send(t + 1).start()

    first = me_tp * half_blocks
    with jax.named_scope("attend2"):
        attend(units_of(first))
    with jax.named_scope("pool2"):
        pool_half(first, carried)

    with jax.named_scope("wait_give"):
        for t in range(tiles):
            partial_send(t).wait_recv()
    with jax.named_scope("keep"):
        for t in range(tiles):
            mine = dot(act[...], wout[:, columns(t)])
            out[:, columns(t)] = (mine + landing[t].astype(F32)).astype(BF16)
    for t in range(tiles):
        partial_send(t).wait_send()
    for c in range(chunks):
        remote_tokens(c).wait_send()
    for step in range(1, n_sp):

        @pl.when(me_sp + step < n_sp)
        def _():
            total_copy(step).wait_send()


    @pl.when(me_sp < n_sp - 1)
    def _():
        halo_keys.wait_send()
        halo_vals.wait_send()
        halo_pool.wait_send()


def shards(n_sp, tokens, gain, wq, wk, wv, sink, wp, wo, wpo):
    rows, half_width = tokens.shape[1:]
    width = 2 * half_width
    heads, head_dim = wq.shape[1:]
    local_kv = wk.shape[1]
    channels = wp.shape[2]
    q_rows, kv_rows = (heads * head_dim, local_kv * head_dim)
    pool_cols = 4 * channels
    blocks = rows // WINDOW
    tiles = width // COLS
    chunks = rows // CHUNK
    dma = pltpu.SemaphoreType.DMA
    flat = lambda w: jnp.transpose(w, (1, 2, 0)).reshape(-1, width)
    hbm = pl.BlockSpec(memory_space=pltpu.HBM)
    vmem = pl.BlockSpec(memory_space=pltpu.VMEM)
    result = pl.pallas_call(
        functools.partial(kernel, n_sp, heads, local_kv, head_dim),
        out_shape=pltpu.VMEM((rows // 2, width), BF16),
        in_specs=[hbm] * 9,
        out_specs=vmem,
        scratch_shapes=[
            pltpu.VMEM((1, width), F32),
            pltpu.SMEM((heads,), F32),
            pltpu.VMEM((WINDOW, PAIR * WINDOW), BF16),
            pltpu.VMEM((2, rows, half_width), BF16),
            pltpu.VMEM((chunks, CHUNK, width), BF16),
            pltpu.VMEM((q_rows + 2 * kv_rows, width), BF16),
            pltpu.VMEM((4 * width, channels), BF16),
            pltpu.VMEM((1024, channels), F32),
            pltpu.VMEM((width, pool_cols), BF16),
            pltpu.VMEM((q_rows + pool_cols, width), BF16),
            pltpu.VMEM((blocks, q_rows, WINDOW), BF16),
            pltpu.VMEM((blocks + 1, WINDOW, kv_rows), BF16),
            pltpu.VMEM((blocks + 1, kv_rows, WINDOW), BF16),
            pltpu.VMEM((rows + WINDOW, pool_cols), BF16),
            pltpu.VMEM((4, WINDOW, 2 * WINDOW), BF16),
            pltpu.VMEM((blocks, 8, channels), F32),
            pltpu.VMEM((n_sp, 8, channels), F32),
            pltpu.VMEM((rows // 2, q_rows + pool_cols), BF16),
            pltpu.VMEM((tiles, rows // 2, COLS), BF16),
            pltpu.VMEM((tiles, rows // 2, COLS), BF16),
            dma((8,)),
            dma((chunks,)),
            dma((chunks,)),
            dma((chunks,)),
            dma((3,)),
            dma((3,)),
            dma((n_sp,)),
            dma((n_sp,)),
            dma((tiles,)),
            dma((tiles,)),
            pltpu.SemaphoreType.REGULAR((n_sp,)),
        ],
        compiler_params=pltpu.CompilerParams(
            collective_id=0, has_side_effects=True, vmem_limit_bytes=67043328 - rows * width - 65536
        ),
    )(
        tokens[0],
        gain.reshape(1, width),
        flat(wq),
        flat(wk),
        flat(wv),
        sink,
        wp.reshape(-1, channels),
        wo.reshape(-1, width),
        wpo.reshape(-1, width),
    )
    return result[None]


def solution(mesh):
    in_specs = (
        P("fs", ("grp", "sp"), "tp"),
        P(),
        P(None, "tp", None),
        P(None, "tp", None),
        P(None, "tp", None),
        P("tp"),
        P(None, None, "tp"),
        P("tp", None, None),
        P(None, "tp", None),
    )
    out_specs = P("fs", ("grp", "sp", "tp"), None)
    return jax.shard_map(
        functools.partial(shards, mesh.shape["sp"]),
        mesh=mesh,
        in_specs=in_specs,
        out_specs=out_specs,
        check_vma=False,
    )
```

```python
import functools

import jax
import jax.numpy as jnp
from jax import lax
from jax.experimental import pallas as pl
from jax.experimental.pallas import tpu as pltpu
from jax.sharding import PartitionSpec as P

MESH = pl.DeviceIdType.MESH
WINDOW = 128
REACHES = (2, 4, 16)
TAIL = 16
CHUNK = 256
COLS = 512
PAIR = 2
F32 = jnp.float32
BF16 = jnp.bfloat16
scope = jax.named_scope


def dot(a, b, dims=((1,), (0,))):
    return lax.dot_general(a, b, (dims, ((), ())), preferred_element_type=F32)


def normalize(low_ref, high_ref, gain, store):
    half_width = low_ref.shape[1]
    low = low_ref[...].astype(F32)
    high = high_ref[...].astype(F32)
    square = jnp.sum(low * low, axis=1, keepdims=True)
    square = square + jnp.sum(high * high, axis=1, keepdims=True)
    inv = lax.rsqrt(square * (0.5 / half_width) + 1e-06)
    low_at, high_at = pl.ds(0, half_width), pl.ds(half_width, half_width)
    store(low_at, (low * inv * gain[:, low_at]).astype(BF16))
    store(high_at, (high * inv * gain[:, high_at]).astype(BF16))


def store_into(ref):
    def store(at, value):
        ref[:, at] = value

    return store


def project_pool(normed, wpool, ext_rows, sums):
    pooled_in = dot(normed[...], wpool[...]).astype(BF16)
    ext_rows[...] = pooled_in
    channels = pooled_in.shape[1] // 4
    last = pooled_in[:, 3 * channels :].astype(F32)
    for j in range(pooled_in.shape[0] // WINDOW):
        summed = jnp.sum(last[j * WINDOW : (j + 1) * WINDOW], axis=0, keepdims=True)
        sums[j] = jnp.broadcast_to(summed, (8, channels))


def mix_kernel(
    n_sp,
    heads,
    local_kv,
    head_dim,
    tokens,
    gain_hbm,
    wq,
    wk,
    wv,
    wp,
    wo,
    wpo,
    sink_hbm,
    act,
    out_left,
    landing_right,
    wout,
    tok,
    normed,
    gain,
    sink,
    wp_raw,
    wp_f32,
    wpool,
    wqkv,
    tri,
    bands,
    qt,
    keys,
    vals,
    ext,
    block_sum,
    totals,
    sending,
    landing_left,
    w_sem,
    tok_sem,
    tok_send,
    tok_recv,
    halo_send,
    halo_recv,
    tot_send,
    tot_recv,
    out_send,
    out_recv,
    ready,
):
    me_sp = lax.axis_index("sp")
    me_tp = lax.axis_index("tp")
    other = 1 - me_tp
    width = wout.shape[1]
    q_rows = heads * head_dim
    kv_rows = local_kv * head_dim
    pool_cols = wpool.shape[1]
    channels = pool_cols // 4
    rows = act.shape[0]
    blocks = rows // WINDOW
    chunks = rows // CHUNK
    per_chunk = CHUNK // WINDOW
    half_rows = rows // 2
    half_blocks = blocks // 2
    tiles = width // COLS
    left_tiles = landing_left.shape[0]
    group = heads // local_kv

    def either(for_zero, for_one):
        return for_zero + me_tp * (for_one - for_zero)

    for index in range(n_sp):
        totals[index] = jnp.zeros((8, channels), F32)
    barrier = pltpu.get_barrier_semaphore()

    @pl.when(me_tp == 1)
    def _():
        pl.semaphore_signal(barrier, inc=1, device_id={"tp": 0}, device_id_type=MESH)

    def local_tokens(c):
        return pltpu.make_async_copy(
            tokens.at[pl.ds(c * CHUNK, CHUNK), :], tok.at[c, me_tp], tok_sem.at[c]
        )

    def remote_tokens(c):
        direct = c == chunks - 1
        return pltpu.make_async_remote_copy(
            src_ref=tokens.at[pl.ds(c * CHUNK, CHUNK), :] if direct else tok.at[c, me_tp],
            dst_ref=tok.at[c, me_tp],
            send_sem=tok_send.at[c],
            recv_sem=tok_recv.at[c],
            device_id={"tp": other},
            device_id_type=MESH,
        )

    load_wp = pltpu.make_async_copy(wp, wp_raw, w_sem.at[0])
    load_gain = pltpu.make_async_copy(gain_hbm, gain, w_sem.at[1])
    loads = [
        pltpu.make_async_copy(wq, wqkv.at[pl.ds(0, q_rows), :], w_sem.at[2]),
        pltpu.make_async_copy(wk, wqkv.at[pl.ds(q_rows, kv_rows), :], w_sem.at[3]),
        pltpu.make_async_copy(wv, wqkv.at[pl.ds(q_rows + kv_rows, kv_rows), :], w_sem.at[4]),
    ]
    load_out = [
        pltpu.make_async_copy(wo, wout.at[pl.ds(0, q_rows), :], w_sem.at[5]),
        pltpu.make_async_copy(wpo, wout.at[pl.ds(q_rows, 4 * channels), :], w_sem.at[6]),
    ]
    load_sink = pltpu.make_async_copy(sink_hbm, sink, w_sem.at[7])
    for c in reversed(range(chunks)):
        local_tokens(c).start()
    load_gain.start()
    load_wp.start(priority=1)
    for load in loads + load_out:
        load.start(priority=1)
    load_sink.start()

    with scope("barrier"):

        @pl.when(me_tp == 0)
        def _():
            pl.semaphore_wait(barrier, 1)
            pl.semaphore_signal(ready.at[0], inc=1, device_id={"tp": 1}, device_id_type=MESH)

        @pl.when(me_tp == 1)
        def _():
            pl.semaphore_wait(ready.at[0], 1)

    remote_tokens(chunks - 1).start()
    for step in range(1, n_sp):

        @pl.when((me_tp == 1) & (me_sp - step >= 0))
        def _():
            pl.semaphore_signal(
                barrier,
                inc=1,
                device_id={"sp": lax.rem(me_sp - step + n_sp, n_sp)},
                device_id_type=MESH,
            )

    target = lax.broadcasted_iota(jnp.int32, (WINDOW, 2 * WINDOW), 0) + WINDOW
    source = lax.broadcasted_iota(jnp.int32, (WINDOW, 2 * WINDOW), 1)
    gap = target - source
    for g, reach in enumerate(REACHES):
        bands[g] = jnp.where((gap >= 0) & (gap < reach), 1.0, 0.0).astype(BF16)
    bands[3] = jnp.where((gap >= 0) & (gap < WINDOW) & (source >= WINDOW), 1.0, 0.0).astype(BF16)
    own_key = lax.broadcasted_iota(jnp.int32, (WINDOW, PAIR * WINDOW), 0) <= lax.rem(
        lax.broadcasted_iota(jnp.int32, (WINDOW, PAIR * WINDOW), 1), jnp.int32(WINDOW)
    )
    tri[...] = jnp.where(own_key, 1.0, 0.0).astype(BF16)
    ext[pl.ds(0, WINDOW - TAIL), :] = jnp.zeros((WINDOW - TAIL, pool_cols), BF16)

    @pl.when(me_sp == 0)
    def _():
        ext[pl.ds(WINDOW - TAIL, TAIL), :] = jnp.zeros((TAIL, pool_cols), BF16)
        keys[0] = jnp.zeros((WINDOW, kv_rows), BF16)
        vals[0] = jnp.zeros((kv_rows, WINDOW), BF16)

    def halo_copy(src, dst, index):
        return pltpu.make_async_remote_copy(
            src_ref=src,
            dst_ref=dst,
            send_sem=halo_send.at[index],
            recv_sem=halo_recv.at[index],
            device_id={"sp": lax.rem(me_sp + 1, n_sp)},
            device_id_type=MESH,
        )

    halos = [
        halo_copy(keys.at[blocks], keys.at[0], 0),
        halo_copy(vals.at[blocks], vals.at[0], 1),
        halo_copy(
            ext.at[pl.ds(WINDOW + rows - TAIL, TAIL), :],
            ext.at[pl.ds(WINDOW - TAIL, TAIL), :],
            2,
        ),
    ]

    def total_copy(step):
        return pltpu.make_async_remote_copy(
            src_ref=totals.at[me_sp],
            dst_ref=totals.at[me_sp],
            send_sem=tot_send.at[step],
            recv_sem=tot_recv.at[step],
            device_id={"sp": lax.rem(me_sp + step, n_sp)},
            device_id_type=MESH,
        )

    scale = head_dim ** (-0.5)

    def qkv(c, source):
        half = wqkv.shape[0] // 2
        low = dot(wqkv[pl.ds(0, half), :], source, ((1,), (1,)))
        high = dot(wqkv[pl.ds(half, half), :], source, ((1,), (1,)))
        split = q_rows - half
        for j in range(per_chunk):
            b = c * per_chunk + j
            at = slice(j * WINDOW, (j + 1) * WINDOW)
            qt[b, pl.ds(0, half), :] = (low[:, at] * scale).astype(BF16)
            qt[b, pl.ds(half, split), :] = (high[:split, at] * scale).astype(BF16)
            keys[b + 1] = high[split : split + kv_rows, at].T.astype(BF16)
            vals[b + 1] = high[split + kv_rows :, at].astype(BF16)

    def ext_chunk(c):
        return ext.at[pl.ds(WINDOW + c * CHUNK, CHUNK), :]

    none = jnp.zeros((head_dim, PAIR * WINDOW), BF16)

    def unit_scores(unit):
        b, h, p, edge = unit
        first_head = h * group + p * PAIR
        q = jnp.concatenate(
            [qt[b, pl.ds((first_head + g) * head_dim, head_dim), :] for g in range(PAIR)],
            axis=1,
        )
        rhs = jnp.concatenate([q if k == h else none for k in range(local_kv)], axis=0)
        return dot(keys[b], rhs), dot(keys[b + 1], rhs)

    def unit_weights(unit, scores):
        b, h, p, edge = unit
        first_head = h * group + p * PAIR
        before, own = scores
        if edge:
            before = before + jnp.where((b == 0) & (me_sp == 0), -jnp.inf, 0.0).astype(F32)
        s = jnp.concatenate(
            [jnp.full((1, WINDOW), sink[first_head + g], F32) for g in range(PAIR)], axis=1
        )
        score = jnp.where(own_key, own, before)
        top = jnp.maximum(jnp.max(score, axis=0, keepdims=True), s)
        expo = jnp.exp(score - top)
        total = jnp.sum(expo, axis=0, keepdims=True) + jnp.exp(s - top)
        weight = (expo * (1.0 / total)).astype(BF16)
        w_own = weight * tri[...]
        return jnp.concatenate([weight - w_own, w_own], axis=0)

    def block_rows(b):
        return pl.ds(pl.multiple_of(b * WINDOW, WINDOW), WINDOW)

    def unit_output(unit, weights):
        b, h, p, edge = unit
        first_head = h * group + p * PAIR
        v_at = pl.ds(h * head_dim, head_dim)
        v = jnp.concatenate([vals[b, v_at, :], vals[b + 1, v_at, :]], axis=1)
        gathered = dot(v, weights)
        stacked = jnp.concatenate(
            [gathered[:, g * WINDOW : (g + 1) * WINDOW] for g in range(PAIR)], axis=0
        )
        act[block_rows(b), pl.ds(first_head * head_dim, PAIR * head_dim)] = stacked.T.astype(BF16)

    ascending = [blocks - 1, 1, 2, 0] + list(range(3, blocks - 1))
    sequence = [either(blocks - 1 - i, ascending[i]) for i in range(blocks)]
    units = [
        (sequence[i], h, p, 0 in (blocks - 1 - i, ascending[i]))
        for i in range(blocks)
        for h in range(local_kv)
        for p in range(group // PAIR)
    ]
    per_block = len(units) // blocks
    scores, weights = {}, {}

    def score(first, count):
        for u in range(first, first + count):
            scores[u] = unit_scores(units[u])

    def soften(first, count):
        for u in range(first, first + count):
            weights[u] = unit_weights(units[u], scores.pop(u))

    def gather(first, count):
        for u in range(first, first + count):
            unit_output(units[u], weights.pop(u))

    def pool(b, groups, carried=None):
        start = pl.multiple_of(b * WINDOW, WINDOW)
        position = me_sp * rows + b * WINDOW + 1
        count = (lax.broadcasted_iota(jnp.int32, (WINDOW, channels), 0) + position).astype(F32)
        for g in groups:
            col = pl.ds(g * channels, channels)
            own = ext[pl.ds(start + WINDOW, WINDOW), col]
            if g < 3:
                sums = dot(bands[g], ext[pl.ds(start, 2 * WINDOW), col])
                denom = jnp.minimum(count, float(REACHES[g]))
            else:
                base = carried
                for earlier in range(blocks):
                    base = base + jnp.where(earlier < b, block_sum[earlier], 0.0)
                sums = dot(bands[3, :, pl.ds(WINDOW, WINDOW)], own) + base[:1]
                denom = count
            pooled = sums * (1.0 / denom) - own.astype(F32)
            act[block_rows(b), pl.ds(q_rows + g * channels, channels)] = pooled.astype(BF16)

    def columns(t):
        return pl.ds(t * COLS, COLS)

    def partial_send(t):
        left = t < left_tiles
        return pltpu.make_async_remote_copy(
            src_ref=sending.at[t],
            dst_ref=landing_left.at[t] if left else landing_right.at[t - left_tiles],
            send_sem=out_send.at[t],
            recv_sem=out_recv.at[t],
            device_id={"tp": other},
            device_id_type=MESH,
        )

    with scope("send_tokens"):
        for c in reversed(range(chunks - 1)):
            local_tokens(c).wait()
            remote_tokens(c).start()
    with scope("wait_wp"):
        load_wp.wait()
    part = wp_f32.shape[0]

    def regroup(i, carry):
        wp_f32[...] = wp_raw[pl.ds(pl.multiple_of(i * part, part), part), :].astype(F32)
        at = pl.ds(pl.multiple_of(i * (part // 4), part // 4), part // 4)
        for g in range(4):
            wpool[at, pl.ds(g * channels, channels)] = wp_f32[
                pl.ds(g, part // 4, stride=4), :
            ].astype(BF16)
        return carry

    def normalize_chunk(c):
        normalize(tok.at[c, 0], tok.at[c, 1], gain, store_into(normed.at[c]))

    with scope("regroup"):
        lax.fori_loop(0, wp_raw.shape[0] // part, regroup, 0)
    with scope("wait_tokens"):
        load_gain.wait()
        local_tokens(chunks - 1).wait()
        remote_tokens(chunks - 1).wait_recv()
    with scope("normalize"):
        normalize_chunk(chunks - 1)
    for c in reversed(range(chunks)):
        if c > 0:
            with scope("wait_tokens"):
                remote_tokens(c - 1).wait_recv()
        with scope("pool_proj"):
            project_pool(
                normed.at[c], wpool, ext_chunk(c), block_sum.at[pl.ds(c * per_chunk, per_chunk)]
            )
            if c > 0:
                normalize_chunk(c - 1)
    all_rows = block_sum[0]
    for b in range(1, blocks):
        all_rows = all_rows + block_sum[b]
    totals[me_sp] = all_rows
    with scope("sp_ready"):

        @pl.when(me_sp < n_sp - 1)
        def _():
            @pl.when(me_tp == 1)
            def _():
                pl.semaphore_wait(barrier, n_sp - 1 - me_sp)
                pl.semaphore_signal(ready.at[1], inc=1, device_id={"tp": 0}, device_id_type=MESH)

            @pl.when(me_tp == 0)
            def _():
                pl.semaphore_wait(ready.at[1], 1)

    for step in range(1, n_sp):

        @pl.when(me_sp + step < n_sp)
        def _():
            total_copy(step).start()

    with scope("wait_wqkv"):
        for load in loads:
            load.wait()
    with scope("qkv_first"):
        qkv(chunks - 1, normed[chunks - 1])

    @pl.when(me_sp < n_sp - 1)
    def _():
        for halo in halos:
            halo.start()

    load_sink.wait()
    give_first = other * half_blocks
    keep_first = me_tp * half_blocks

    def half_of(first):
        return act[pl.ds(pl.multiple_of(first * WINDOW, WINDOW), half_rows), :]

    quarter = COLS // 2

    def give(t, part):
        at = pl.ds(t * COLS + part * quarter, quarter)
        sending[t, :, pl.ds(part * quarter, quarter)] = dot(
            half_of(give_first), wout[:, at]
        ).astype(BF16)

    for i in range(1, chunks):
        c = either(chunks - 1 - i, i - 1)
        with scope("qkv_rest"):
            first = (i - 1) * per_block
            score(first, per_block)
            qkv(c, normed[c])
            soften(first, per_block)
            gather(first, per_block)
    with scope("attend_a"):
        first = (chunks - 1) * per_block
        score(first, per_block)
        pairs = [(i, g) for i in range(half_blocks) for g in range(3)]

    def wait_halo(tp):
        with scope("wait_halo"):

            @pl.when((me_sp > 0) & (me_tp == tp))
            def _():
                for halo in halos:
                    halo.wait_recv()

    wait_halo(1)
    with scope("attend_b"):
        soften(first, per_block)
        score(first + per_block, per_block)
        gather(first, per_block)
        for i, g in pairs:
            pool(give_first + i, (g,))
        soften(first + per_block, per_block)
        gather(first + per_block, per_block)
    with scope("wait_totals"):
        for step in range(1, n_sp):

            @pl.when(me_sp - step >= 0)
            def _():
                total_copy(step).wait_recv()

    carried = jnp.zeros((8, channels), F32)
    for index in range(n_sp):
        carried = carried + jnp.where(index < me_sp, totals[index], 0.0)
    first = first + 2 * per_block
    left = len(units) - first
    with scope("pool_b"):
        score(first, left // tiles)
        for i in range(half_blocks):
            pool(give_first + i, (3,), carried)

    keep_pieces = [(i, g) for i in reversed(range(half_blocks)) for g in range(4)]
    for load in load_out:
        load.wait()
    for t in range(tiles):
        if t == 1:
            wait_halo(0)
        with scope("give"):
            lo, hi = first + t * left // tiles, first + (t + 1) * left // tiles
            for part in range(2):
                give(t, part)
            soften(lo, hi - lo)
            if t < tiles - 1:
                score(hi, first + (t + 2) * left // tiles - hi)
            gather(lo, hi - lo)
            at = [len(keep_pieces) * k // tiles for k in (t, t + 1)]
            for i, g in keep_pieces[at[0] : at[1]]:
                pool(keep_first + i, (g,), carried)
        partial_send(t).start()
    with scope("wait_give"):
        for t in range(left_tiles):
            partial_send(t).wait_recv()
    with scope("keep"):
        for t in range(left_tiles):
            mine = dot(half_of(keep_first), wout[:, columns(t)])
            out_left[:, columns(t)] = (mine + landing_left[t].astype(F32)).astype(BF16)
    with scope("end_mix"):
        for t in range(left_tiles, tiles):
            partial_send(t).wait_recv()
        for t in range(tiles):
            partial_send(t).wait_send()
        for c in range(chunks):
            remote_tokens(c).wait_send()
        for step in range(1, n_sp):

            @pl.when(me_sp + step < n_sp)
            def _():
                total_copy(step).wait_send()

        @pl.when(me_sp < n_sp - 1)
        def _():
            for halo in halos:
                halo.wait_send()


def finish_kernel(act, wout, out_left, landing_right, out, out_right, sem):
    me_tp = lax.axis_index("tp")
    half_rows, left_width = out_left.shape
    right_tiles = landing_right.shape[0]
    left = pltpu.make_async_copy(out_left, out.at[:, pl.ds(0, left_width)], sem.at[0])
    left.start()

    def right(t):
        at = pl.ds(left_width + t * COLS, COLS)
        return pltpu.make_async_copy(out_right.at[t], out.at[:, at], sem.at[1 + t])

    mine = act[pl.ds(pl.multiple_of(me_tp * half_rows, half_rows), half_rows), :]
    for t in range(right_tiles):
        at = pl.ds(left_width + t * COLS, COLS)
        out_right[t] = (dot(mine, wout[:, at]) + landing_right[t].astype(F32)).astype(BF16)
        right(t).start()
    left.wait()
    for t in range(right_tiles):
        right(t).wait()


def shards(n_sp, tokens, gain, wq, wk, wv, sink, wp, wo, wpo):
    rows, half_width = tokens.shape[1:]
    width = 2 * half_width
    heads, head_dim = wq.shape[1:]
    local_kv = wk.shape[1]
    channels = wp.shape[2]
    q_rows, kv_rows = (heads * head_dim, local_kv * head_dim)
    pool_cols = 4 * channels
    blocks = rows // WINDOW
    tiles = width // COLS
    left_tiles = tiles - 1
    chunks = rows // CHUNK
    per_chunk = CHUNK // WINDOW
    half_rows = rows // 2
    dma = pltpu.SemaphoreType.DMA
    flat = lambda w: jnp.transpose(w, (1, 2, 0)).reshape(-1, width)
    hbm = pl.BlockSpec(memory_space=pltpu.HBM)
    vmem = pl.BlockSpec(memory_space=pltpu.VMEM)

    mixed = [
        ((rows, q_rows + pool_cols), BF16),
        ((half_rows, left_tiles * COLS), BF16),
        ((tiles - left_tiles, half_rows, COLS), BF16),
        ((q_rows + pool_cols, width), BF16),
    ]
    size = lambda shapes: sum(
        functools.reduce(lambda a, b: a * b, s) * jnp.dtype(d).itemsize for s, d in shapes
    )
    spare = 67043328 - 262144
    act, out_left, landing_right, wout = pl.pallas_call(
        functools.partial(mix_kernel, n_sp, heads, local_kv, head_dim),
        out_shape=[pltpu.VMEM(s, d) for s, d in mixed],
        in_specs=[hbm] * 9,
        out_specs=[vmem] * len(mixed),
        scratch_shapes=[
            pltpu.VMEM((chunks, 2, CHUNK, half_width), BF16),
            pltpu.VMEM((chunks, CHUNK, width), BF16),
            pltpu.VMEM((1, width), F32),
            pltpu.SMEM((heads,), F32),
            pltpu.VMEM((4 * width, channels), BF16),
            pltpu.VMEM((1024, channels), F32),
            pltpu.VMEM((width, pool_cols), BF16),
            pltpu.VMEM((q_rows + 2 * kv_rows, width), BF16),
            pltpu.VMEM((WINDOW, PAIR * WINDOW), BF16),
            pltpu.VMEM((4, WINDOW, 2 * WINDOW), BF16),
            pltpu.VMEM((blocks, q_rows, WINDOW), BF16),
            pltpu.VMEM((blocks + 1, WINDOW, kv_rows), BF16),
            pltpu.VMEM((blocks + 1, kv_rows, WINDOW), BF16),
            pltpu.VMEM((rows + WINDOW, pool_cols), BF16),
            pltpu.VMEM((blocks, 8, channels), F32),
            pltpu.VMEM((n_sp, 8, channels), F32),
            pltpu.VMEM((tiles, half_rows, COLS), BF16),
            pltpu.VMEM((left_tiles, half_rows, COLS), BF16),
            dma((8,)),
            dma((chunks,)),
            dma((chunks,)),
            dma((chunks,)),
            dma((3,)),
            dma((3,)),
            dma((n_sp,)),
            dma((n_sp,)),
            dma((tiles,)),
            dma((tiles,)),
            pltpu.SemaphoreType.REGULAR((2,)),
        ],
        compiler_params=pltpu.CompilerParams(
            collective_id=0, has_side_effects=True, vmem_limit_bytes=spare - size(mixed)
        ),
    )(
        tokens[0],
        gain.reshape(1, width),
        flat(wq),
        flat(wk),
        flat(wv),
        wp.reshape(-1, channels),
        wo.reshape(-1, width),
        wpo.reshape(-1, width),
        sink,
    )
    result = pl.pallas_call(
        finish_kernel,
        out_shape=jax.ShapeDtypeStruct((half_rows, width), BF16),
        in_specs=[vmem] * 4,
        out_specs=hbm,
        scratch_shapes=[
            pltpu.VMEM((tiles - left_tiles, half_rows, COLS), BF16),
            dma((1 + tiles - left_tiles,)),
        ],
        compiler_params=pltpu.CompilerParams(vmem_limit_bytes=spare // 3),
    )(act, wout, out_left, landing_right)
    return result[None]


def solution(mesh):
    in_specs = (
        P("fs", ("grp", "sp"), "tp"),
        P(),
        P(None, "tp", None),
        P(None, "tp", None),
        P(None, "tp", None),
        P("tp"),
        P(None, None, "tp"),
        P("tp", None, None),
        P(None, "tp", None),
    )
    out_specs = P("fs", ("grp", "sp", "tp"), None)
    return jax.shard_map(
        functools.partial(shards, mesh.shape["sp"]),
        mesh=mesh,
        in_specs=in_specs,
        out_specs=out_specs,
        check_vma=False,
    )
```

```python
import functools

import jax
import jax.numpy as jnp
from jax import lax
from jax.experimental import pallas as pl
from jax.experimental.pallas import tpu as pltpu
from jax.sharding import PartitionSpec as P

MESH = pl.DeviceIdType.MESH
WINDOW = 128
REACHES = (2, 4, 16)
TAIL = 16
CHUNK = 256
COLS = 512
PAIR = 2
F32 = jnp.float32
BF16 = jnp.bfloat16
scope = jax.named_scope


def dot(a, b, dims=((1,), (0,))):
    return lax.dot_general(a, b, (dims, ((), ())), preferred_element_type=F32)


def normalize(low_ref, high_ref, gain, store):
    half_width = low_ref.shape[1]
    low = low_ref[...].astype(F32)
    high = high_ref[...].astype(F32)
    square = jnp.sum(low * low, axis=1, keepdims=True)
    square = square + jnp.sum(high * high, axis=1, keepdims=True)
    inv = lax.rsqrt(square * (0.5 / half_width) + 1e-06)
    low_at, high_at = pl.ds(0, half_width), pl.ds(half_width, half_width)
    store(low_at, (low * inv * gain[:, low_at]).astype(BF16))
    store(high_at, (high * inv * gain[:, high_at]).astype(BF16))


def store_into(ref):
    def store(at, value):
        ref[:, at] = value

    return store


def project_pool(normed, wpool, ext_rows, sums):
    pooled_in = dot(normed[...], wpool[...]).astype(BF16)
    ext_rows[...] = pooled_in
    channels = pooled_in.shape[1] // 4
    last = pooled_in[:, 3 * channels :].astype(F32)
    for j in range(pooled_in.shape[0] // WINDOW):
        summed = jnp.sum(last[j * WINDOW : (j + 1) * WINDOW], axis=0, keepdims=True)
        sums[j] = jnp.broadcast_to(summed, (8, channels))


def mix_kernel(
    n_sp,
    heads,
    local_kv,
    head_dim,
    tokens,
    gain_hbm,
    wq,
    wk,
    wv,
    wp,
    wo,
    wpo,
    sink_hbm,
    act,
    out_left,
    landing_right,
    wout,
    tok,
    normed,
    gain,
    sink,
    wp_raw,
    wp_f32,
    wpool,
    wqkv,
    tri,
    bands,
    qt,
    keys,
    vals,
    ext,
    block_sum,
    totals,
    sending,
    landing_left,
    w_sem,
    tok_sem,
    tok_send,
    tok_recv,
    halo_send,
    halo_recv,
    tot_send,
    tot_recv,
    out_send,
    out_recv,
    ready,
):
    me_sp = lax.axis_index("sp")
    me_tp = lax.axis_index("tp")
    other = 1 - me_tp
    width = wout.shape[1]
    q_rows = heads * head_dim
    kv_rows = local_kv * head_dim
    pool_cols = wpool.shape[1]
    channels = pool_cols // 4
    rows = act.shape[0]
    blocks = rows // WINDOW
    chunks = rows // CHUNK
    per_chunk = CHUNK // WINDOW
    half_rows = rows // 2
    half_blocks = blocks // 2
    tiles = width // COLS
    left_tiles = landing_left.shape[0]
    group = heads // local_kv

    def either(for_zero, for_one):
        return for_zero + me_tp * (for_one - for_zero)

    for index in range(n_sp):
        totals[index] = jnp.zeros((8, channels), F32)
    barrier = pltpu.get_barrier_semaphore()

    @pl.when(me_tp == 1)
    def _():
        pl.semaphore_signal(barrier, inc=1, device_id={"tp": 0}, device_id_type=MESH)

    def local_tokens(c):
        return pltpu.make_async_copy(
            tokens.at[pl.ds(c * CHUNK, CHUNK), :], tok.at[c, me_tp], tok_sem.at[c]
        )

    def remote_tokens(c):
        direct = c == chunks - 1
        return pltpu.make_async_remote_copy(
            src_ref=tokens.at[pl.ds(c * CHUNK, CHUNK), :] if direct else tok.at[c, me_tp],
            dst_ref=tok.at[c, me_tp],
            send_sem=tok_send.at[c],
            recv_sem=tok_recv.at[c],
            device_id={"tp": other},
            device_id_type=MESH,
        )

    load_wp = pltpu.make_async_copy(wp, wp_raw, w_sem.at[0])
    load_gain = pltpu.make_async_copy(gain_hbm, gain, w_sem.at[1])
    loads = [
        pltpu.make_async_copy(wq, wqkv.at[pl.ds(0, q_rows), :], w_sem.at[2]),
        pltpu.make_async_copy(wk, wqkv.at[pl.ds(q_rows, kv_rows), :], w_sem.at[3]),
        pltpu.make_async_copy(wv, wqkv.at[pl.ds(q_rows + kv_rows, kv_rows), :], w_sem.at[4]),
    ]
    load_out = [
        pltpu.make_async_copy(wo, wout.at[pl.ds(0, q_rows), :], w_sem.at[5]),
        pltpu.make_async_copy(wpo, wout.at[pl.ds(q_rows, 4 * channels), :], w_sem.at[6]),
    ]
    load_sink = pltpu.make_async_copy(sink_hbm, sink, w_sem.at[7])
    for c in reversed(range(chunks)):
        local_tokens(c).start()
    load_gain.start()
    for load in loads + [load_wp] + load_out:
        load.start(priority=1)
    load_sink.start()

    with scope("barrier"):

        @pl.when(me_tp == 0)
        def _():
            pl.semaphore_wait(barrier, 1)
            pl.semaphore_signal(ready.at[0], inc=1, device_id={"tp": 1}, device_id_type=MESH)

        @pl.when(me_tp == 1)
        def _():
            pl.semaphore_wait(ready.at[0], 1)

    remote_tokens(chunks - 1).start()
    for step in range(1, n_sp):

        @pl.when((me_tp == 1) & (me_sp - step >= 0))
        def _():
            pl.semaphore_signal(
                barrier,
                inc=1,
                device_id={"sp": lax.rem(me_sp - step + n_sp, n_sp)},
                device_id_type=MESH,
            )

    target = lax.broadcasted_iota(jnp.int32, (WINDOW, 2 * WINDOW), 0) + WINDOW
    source = lax.broadcasted_iota(jnp.int32, (WINDOW, 2 * WINDOW), 1)
    gap = target - source
    for g, reach in enumerate(REACHES):
        bands[g] = jnp.where((gap >= 0) & (gap < reach), 1.0, 0.0).astype(BF16)
    bands[3] = jnp.where((gap >= 0) & (gap < WINDOW) & (source >= WINDOW), 1.0, 0.0).astype(BF16)
    own_key = lax.broadcasted_iota(jnp.int32, (WINDOW, PAIR * WINDOW), 0) <= lax.rem(
        lax.broadcasted_iota(jnp.int32, (WINDOW, PAIR * WINDOW), 1), jnp.int32(WINDOW)
    )
    tri[...] = jnp.where(own_key, 1.0, 0.0).astype(BF16)
    ext[pl.ds(0, WINDOW - TAIL), :] = jnp.zeros((WINDOW - TAIL, pool_cols), BF16)

    @pl.when(me_sp == 0)
    def _():
        ext[pl.ds(WINDOW - TAIL, TAIL), :] = jnp.zeros((TAIL, pool_cols), BF16)
        keys[0] = jnp.zeros((WINDOW, kv_rows), BF16)
        vals[0] = jnp.zeros((kv_rows, WINDOW), BF16)

    def halo_copy(src, dst, index):
        return pltpu.make_async_remote_copy(
            src_ref=src,
            dst_ref=dst,
            send_sem=halo_send.at[index],
            recv_sem=halo_recv.at[index],
            device_id={"sp": lax.rem(me_sp + 1, n_sp)},
            device_id_type=MESH,
        )

    halos = [
        halo_copy(keys.at[blocks], keys.at[0], 0),
        halo_copy(vals.at[blocks], vals.at[0], 1),
        halo_copy(
            ext.at[pl.ds(WINDOW + rows - TAIL, TAIL), :],
            ext.at[pl.ds(WINDOW - TAIL, TAIL), :],
            2,
        ),
    ]

    def total_copy(step):
        return pltpu.make_async_remote_copy(
            src_ref=totals.at[me_sp],
            dst_ref=totals.at[me_sp],
            send_sem=tot_send.at[step],
            recv_sem=tot_recv.at[step],
            device_id={"sp": lax.rem(me_sp + step, n_sp)},
            device_id_type=MESH,
        )

    scale = head_dim ** (-0.5)

    def qkv(c, source):
        half = wqkv.shape[0] // 2
        low = dot(wqkv[pl.ds(0, half), :], source, ((1,), (1,)))
        high = dot(wqkv[pl.ds(half, half), :], source, ((1,), (1,)))
        split = q_rows - half
        for j in range(per_chunk):
            b = c * per_chunk + j
            at = slice(j * WINDOW, (j + 1) * WINDOW)
            qt[b, pl.ds(0, half), :] = (low[:, at] * scale).astype(BF16)
            qt[b, pl.ds(half, split), :] = (high[:split, at] * scale).astype(BF16)
            keys[b + 1] = high[split : split + kv_rows, at].T.astype(BF16)
            vals[b + 1] = high[split + kv_rows :, at].astype(BF16)

    def ext_chunk(c):
        return ext.at[pl.ds(WINDOW + c * CHUNK, CHUNK), :]

    none = jnp.zeros((head_dim, PAIR * WINDOW), BF16)

    def unit_scores(unit):
        b, h, p, edge = unit
        first_head = h * group + p * PAIR
        q = jnp.concatenate(
            [qt[b, pl.ds((first_head + g) * head_dim, head_dim), :] for g in range(PAIR)],
            axis=1,
        )
        rhs = jnp.concatenate([q if k == h else none for k in range(local_kv)], axis=0)
        return dot(keys[b], rhs), dot(keys[b + 1], rhs)

    def unit_weights(unit, scores):
        b, h, p, edge = unit
        first_head = h * group + p * PAIR
        before, own = scores
        if edge:
            before = before + jnp.where((b == 0) & (me_sp == 0), -jnp.inf, 0.0).astype(F32)
        s = jnp.concatenate(
            [jnp.full((1, WINDOW), sink[first_head + g], F32) for g in range(PAIR)], axis=1
        )
        score = jnp.where(own_key, own, before)
        top = jnp.maximum(jnp.max(score, axis=0, keepdims=True), s)
        expo = jnp.exp(score - top)
        total = jnp.sum(expo, axis=0, keepdims=True) + jnp.exp(s - top)
        weight = (expo * (1.0 / total)).astype(BF16)
        w_own = weight * tri[...]
        return jnp.concatenate([weight - w_own, w_own], axis=0)

    def block_rows(b):
        return pl.ds(pl.multiple_of(b * WINDOW, WINDOW), WINDOW)

    def unit_output(unit, weights):
        b, h, p, edge = unit
        first_head = h * group + p * PAIR
        v_at = pl.ds(h * head_dim, head_dim)
        v = jnp.concatenate([vals[b, v_at, :], vals[b + 1, v_at, :]], axis=1)
        gathered = dot(v, weights)
        stacked = jnp.concatenate(
            [gathered[:, g * WINDOW : (g + 1) * WINDOW] for g in range(PAIR)], axis=0
        )
        act[block_rows(b), pl.ds(first_head * head_dim, PAIR * head_dim)] = stacked.T.astype(BF16)

    ascending = [blocks - 1, 1, 0] + list(range(2, blocks - 1))
    sequence = [either(blocks - 1 - i, ascending[i]) for i in range(blocks)]
    units = [
        (sequence[i], h, p, 0 in (blocks - 1 - i, ascending[i]))
        for i in range(blocks)
        for h in range(local_kv)
        for p in range(group // PAIR)
    ]
    per_block = len(units) // blocks
    scores, weights = {}, {}

    def score(first, count):
        for u in range(first, first + count):
            scores[u] = unit_scores(units[u])

    def soften(first, count):
        for u in range(first, first + count):
            weights[u] = unit_weights(units[u], scores.pop(u))

    def gather(first, count):
        for u in range(first, first + count):
            unit_output(units[u], weights.pop(u))

    def pool(b, groups, carried=None):
        start = pl.multiple_of(b * WINDOW, WINDOW)
        position = me_sp * rows + b * WINDOW + 1
        count = (lax.broadcasted_iota(jnp.int32, (WINDOW, channels), 0) + position).astype(F32)
        for g in groups:
            col = pl.ds(g * channels, channels)
            own = ext[pl.ds(start + WINDOW, WINDOW), col]
            if g < 3:
                sums = dot(bands[g], ext[pl.ds(start, 2 * WINDOW), col])
                denom = jnp.minimum(count, float(REACHES[g]))
            else:
                base = carried
                for earlier in range(blocks):
                    base = base + jnp.where(earlier < b, block_sum[earlier], 0.0)
                sums = dot(bands[3, :, pl.ds(WINDOW, WINDOW)], own) + base[:1]
                denom = count
            pooled = sums * (1.0 / denom) - own.astype(F32)
            act[block_rows(b), pl.ds(q_rows + g * channels, channels)] = pooled.astype(BF16)

    def columns(t):
        return pl.ds(t * COLS, COLS)

    def partial_send(t):
        left = t < left_tiles
        return pltpu.make_async_remote_copy(
            src_ref=sending.at[t],
            dst_ref=landing_left.at[t] if left else landing_right.at[t - left_tiles],
            send_sem=out_send.at[t],
            recv_sem=out_recv.at[t],
            device_id={"tp": other},
            device_id_type=MESH,
        )

    with scope("send_tokens"):
        for c in reversed(range(chunks - 1)):
            local_tokens(c).wait()
            remote_tokens(c).start()
    part = 4 * CHUNK

    def regroup(i):
        rows_at = pl.ds(i * part, part)
        wp_f32[rows_at, :] = wp_raw[rows_at, :].astype(F32)
        for g in range(4):
            wpool[pl.ds(i * CHUNK, CHUNK), pl.ds(g * channels, channels)] = wp_f32[
                pl.ds(i * part + g, CHUNK, stride=4), :
            ].astype(BF16)

    def normalize_chunk(c):
        normalize(tok.at[c, 0], tok.at[c, 1], gain, store_into(normed.at[c]))

    with scope("wait_tokens"):
        load_gain.wait()
        local_tokens(chunks - 1).wait()
        remote_tokens(chunks - 1).wait_recv()
    with scope("normalize"):
        normalize_chunk(chunks - 1)
    def pool_chunk(c):
        project_pool(
            normed.at[c], wpool, ext_chunk(c), block_sum.at[pl.ds(c * per_chunk, per_chunk)]
        )

    with scope("wait_wqkv"):
        for load in loads:
            load.wait()
    with scope("wait_wp"):
        load_wp.wait()
        remote_tokens(chunks - 2).wait_recv()
    with scope("first"):
        qkv(chunks - 1, normed[chunks - 1])
        for i in range(wp_raw.shape[0] // part):
            regroup(i)
        normalize_chunk(chunks - 2)
        pool_chunk(chunks - 1)
    with scope("sp_ready"):

        @pl.when(me_sp < n_sp - 1)
        def _():
            @pl.when(me_tp == 1)
            def _():
                pl.semaphore_wait(barrier, n_sp - 1 - me_sp)
                pl.semaphore_signal(ready.at[1], inc=1, device_id={"tp": 0}, device_id_type=MESH)

            @pl.when(me_tp == 0)
            def _():
                pl.semaphore_wait(ready.at[1], 1)

    @pl.when(me_sp < n_sp - 1)
    def _():
        for halo in halos:
            halo.start()

    with scope("wait_tokens"):
        for c in reversed(range(chunks - 2)):
            remote_tokens(c).wait_recv()
    with scope("pool_proj"):
        for c in reversed(range(chunks - 1)):
            pool_chunk(c)
            if c > 0:
                normalize_chunk(c - 1)
        all_rows = block_sum[0]
        for b in range(1, blocks):
            all_rows = all_rows + block_sum[b]
        totals[me_sp] = all_rows

    for step in range(1, n_sp):

        @pl.when(me_sp + step < n_sp)
        def _():
            total_copy(step).start()

    load_sink.wait()
    give_first = other * half_blocks
    keep_first = me_tp * half_blocks

    def half_of(first):
        return act[pl.ds(pl.multiple_of(first * WINDOW, WINDOW), half_rows), :]

    def give(t):
        sending[t] = dot(half_of(give_first), wout[:, columns(t)]).astype(BF16)

    def wait_halo(tp):
        with scope("wait_halo"):

            @pl.when((me_sp > 0) & (me_tp == tp))
            def _():
                for halo in halos:
                    halo.wait_recv()

    first = 0
    for i in range(1, chunks):
        c = either(chunks - 1 - i, i - 1)
        count = per_block * i
        if i == chunks - 1:
            wait_halo(1)
        with scope("qkv_rest"):
            score(first, count)
            soften(first, count)
            qkv(c, normed[c])
            gather(first, count)
        first += count

    with scope("attend_a"):
        score(first, per_block)
        soften(first, per_block)
        for i in range(half_blocks):
            for g in range(3):
                pool(give_first + i, (g,))
        gather(first, per_block)
    first += per_block
    with scope("wait_totals"):
        for step in range(1, n_sp):

            @pl.when(me_sp - step >= 0)
            def _():
                total_copy(step).wait_recv()

    carried = jnp.zeros((8, channels), F32)
    for index in range(n_sp):
        carried = carried + jnp.where(index < me_sp, totals[index], 0.0)
    left = len(units) - first
    with scope("pool_b"):
        score(first, left // tiles)
        for i in range(half_blocks):
            pool(give_first + i, (3,), carried)

    keep_pieces = [(i, g) for i in reversed(range(half_blocks)) for g in range(4)]
    for load in load_out:
        load.wait()
    for t in range(tiles):
        if t == 1:
            wait_halo(0)
        with scope("give"):
            lo, hi = first + t * left // tiles, first + (t + 1) * left // tiles
            soften(lo, hi - lo)
            give(t)
            gather(lo, hi - lo)
            if t < tiles - 1:
                score(hi, first + (t + 2) * left // tiles - hi)
            at = [len(keep_pieces) * k // tiles for k in (t, t + 1)]
            for i, g in keep_pieces[at[0] : at[1]]:
                pool(keep_first + i, (g,), carried)
        partial_send(t).start()
    with scope("wait_give"):
        for t in range(left_tiles):
            partial_send(t).wait_recv()
    with scope("keep"):
        for t in range(left_tiles):
            mine = dot(half_of(keep_first), wout[:, columns(t)])
            out_left[:, columns(t)] = (mine + landing_left[t].astype(F32)).astype(BF16)
    with scope("end_mix"):
        for t in range(left_tiles, tiles):
            partial_send(t).wait_recv()
        for t in range(tiles):
            partial_send(t).wait_send()
        for c in range(chunks):
            remote_tokens(c).wait_send()
        for step in range(1, n_sp):

            @pl.when(me_sp + step < n_sp)
            def _():
                total_copy(step).wait_send()

        @pl.when(me_sp < n_sp - 1)
        def _():
            for halo in halos:
                halo.wait_send()


def finish_kernel(act, wout, out_left, landing_right, out, out_right, sem):
    me_tp = lax.axis_index("tp")
    half_rows, left_width = out_left.shape
    right_tiles = landing_right.shape[0]
    left = pltpu.make_async_copy(out_left, out.at[:, pl.ds(0, left_width)], sem.at[0])
    left.start()

    def right(t):
        at = pl.ds(left_width + t * COLS, COLS)
        return pltpu.make_async_copy(out_right.at[t], out.at[:, at], sem.at[1 + t])

    mine = act[pl.ds(pl.multiple_of(me_tp * half_rows, half_rows), half_rows), :]
    for t in range(right_tiles):
        at = pl.ds(left_width + t * COLS, COLS)
        out_right[t] = (dot(mine, wout[:, at]) + landing_right[t].astype(F32)).astype(BF16)
        right(t).start()
    left.wait()
    for t in range(right_tiles):
        right(t).wait()


def shards(n_sp, tokens, gain, wq, wk, wv, sink, wp, wo, wpo):
    rows, half_width = tokens.shape[1:]
    width = 2 * half_width
    heads, head_dim = wq.shape[1:]
    local_kv = wk.shape[1]
    channels = wp.shape[2]
    q_rows, kv_rows = (heads * head_dim, local_kv * head_dim)
    pool_cols = 4 * channels
    blocks = rows // WINDOW
    tiles = width // COLS
    left_tiles = tiles - 1
    chunks = rows // CHUNK
    per_chunk = CHUNK // WINDOW
    half_rows = rows // 2
    dma = pltpu.SemaphoreType.DMA
    flat = lambda w: jnp.transpose(w, (1, 2, 0)).reshape(-1, width)
    hbm = pl.BlockSpec(memory_space=pltpu.HBM)
    vmem = pl.BlockSpec(memory_space=pltpu.VMEM)

    mixed = [
        ((rows, q_rows + pool_cols), BF16),
        ((half_rows, left_tiles * COLS), BF16),
        ((tiles - left_tiles, half_rows, COLS), BF16),
        ((q_rows + pool_cols, width), BF16),
    ]
    size = lambda shapes: sum(
        functools.reduce(lambda a, b: a * b, s) * jnp.dtype(d).itemsize for s, d in shapes
    )
    spare = 67043328 - 262144
    act, out_left, landing_right, wout = pl.pallas_call(
        functools.partial(mix_kernel, n_sp, heads, local_kv, head_dim),
        out_shape=[pltpu.VMEM(s, d) for s, d in mixed],
        in_specs=[hbm] * 9,
        out_specs=[vmem] * len(mixed),
        scratch_shapes=[
            pltpu.VMEM((chunks, 2, CHUNK, half_width), BF16),
            pltpu.VMEM((chunks, CHUNK, width), BF16),
            pltpu.VMEM((1, width), F32),
            pltpu.SMEM((heads,), F32),
            pltpu.VMEM((4 * width, channels), BF16),
            pltpu.VMEM((4 * width, channels), F32),
            pltpu.VMEM((width, pool_cols), BF16),
            pltpu.VMEM((q_rows + 2 * kv_rows, width), BF16),
            pltpu.VMEM((WINDOW, PAIR * WINDOW), BF16),
            pltpu.VMEM((4, WINDOW, 2 * WINDOW), BF16),
            pltpu.VMEM((blocks, q_rows, WINDOW), BF16),
            pltpu.VMEM((blocks + 1, WINDOW, kv_rows), BF16),
            pltpu.VMEM((blocks + 1, kv_rows, WINDOW), BF16),
            pltpu.VMEM((rows + WINDOW, pool_cols), BF16),
            pltpu.VMEM((blocks, 8, channels), F32),
            pltpu.VMEM((n_sp, 8, channels), F32),
            pltpu.VMEM((tiles, half_rows, COLS), BF16),
            pltpu.VMEM((left_tiles, half_rows, COLS), BF16),
            dma((8,)),
            dma((chunks,)),
            dma((chunks,)),
            dma((chunks,)),
            dma((3,)),
            dma((3,)),
            dma((n_sp,)),
            dma((n_sp,)),
            dma((tiles,)),
            dma((tiles,)),
            pltpu.SemaphoreType.REGULAR((2,)),
        ],
        compiler_params=pltpu.CompilerParams(
            collective_id=0, has_side_effects=True, vmem_limit_bytes=spare - size(mixed)
        ),
    )(
        tokens[0],
        gain.reshape(1, width),
        flat(wq),
        flat(wk),
        flat(wv),
        wp.reshape(-1, channels),
        wo.reshape(-1, width),
        wpo.reshape(-1, width),
        sink,
    )
    result = pl.pallas_call(
        finish_kernel,
        out_shape=jax.ShapeDtypeStruct((half_rows, width), BF16),
        in_specs=[vmem] * 4,
        out_specs=hbm,
        scratch_shapes=[
            pltpu.VMEM((tiles - left_tiles, half_rows, COLS), BF16),
            dma((1 + tiles - left_tiles,)),
        ],
        compiler_params=pltpu.CompilerParams(vmem_limit_bytes=spare // 3),
    )(act, wout, out_left, landing_right)
    return result[None]


def solution(mesh):
    in_specs = (
        P("fs", ("grp", "sp"), "tp"),
        P(),
        P(None, "tp", None),
        P(None, "tp", None),
        P(None, "tp", None),
        P("tp"),
        P(None, None, "tp"),
        P("tp", None, None),
        P(None, "tp", None),
    )
    out_specs = P("fs", ("grp", "sp", "tp"), None)
    return jax.shard_map(
        functools.partial(shards, mesh.shape["sp"]),
        mesh=mesh,
        in_specs=in_specs,
        out_specs=out_specs,
        check_vma=False,
    )
```

```python
import functools

import jax
import jax.numpy as jnp
from jax import lax
from jax.experimental import pallas as pl
from jax.experimental.pallas import tpu as pltpu
from jax.sharding import PartitionSpec as P

MESH = pl.DeviceIdType.MESH
WINDOW = 128
REACHES = (2, 4, 16)
TAIL = 16
CHUNK = 256
COLS = 512
PAIR = 2
LEAD_PARTS = 2
F32 = jnp.float32
BF16 = jnp.bfloat16
scope = jax.named_scope


def dot(a, b, dims=((1,), (0,))):
    return lax.dot_general(a, b, (dims, ((), ())), preferred_element_type=F32)


def normalize(low_ref, high_ref, gain, store):
    half_width = low_ref.shape[1]
    low = low_ref[...].astype(F32)
    high = high_ref[...].astype(F32)
    square = jnp.sum(low * low, axis=1, keepdims=True)
    square = square + jnp.sum(high * high, axis=1, keepdims=True)
    inv = lax.rsqrt(square * (0.5 / half_width) + 1e-06)
    low_at, high_at = pl.ds(0, half_width), pl.ds(half_width, half_width)
    store(low_at, (low * inv * gain[:, low_at]).astype(BF16))
    store(high_at, (high * inv * gain[:, high_at]).astype(BF16))


def store_into(ref):
    def store(at, value):
        ref[:, at] = value

    return store


def project_pool(normed, wpool, ext_rows, sums):
    pooled_in = dot(normed[...], wpool[...]).astype(BF16)
    ext_rows[...] = pooled_in
    channels = pooled_in.shape[1] // 4
    last = pooled_in[:, 3 * channels :].astype(F32)
    for j in range(pooled_in.shape[0] // WINDOW):
        summed = jnp.sum(last[j * WINDOW : (j + 1) * WINDOW], axis=0, keepdims=True)
        sums[j] = jnp.broadcast_to(summed, (8, channels))


def mix_kernel(
    n_sp,
    heads,
    local_kv,
    head_dim,
    tokens,
    gain_hbm,
    wq,
    wk,
    wv,
    wp,
    wo,
    wpo,
    sink_hbm,
    act,
    out_left,
    landing_right,
    wout,
    tok,
    normed,
    gain,
    sink,
    wp_raw,
    wp_f32,
    wpool,
    wqkv,
    tri,
    bands,
    qt,
    keys,
    vals,
    ext,
    block_sum,
    totals,
    sending,
    landing_left,
    w_sem,
    tok_sem,
    tok_send,
    tok_recv,
    halo_send,
    halo_recv,
    tot_send,
    tot_recv,
    out_send,
    out_recv,
    ready,
):
    me_sp = lax.axis_index("sp")
    me_tp = lax.axis_index("tp")
    other = 1 - me_tp
    width = wout.shape[1]
    q_rows = heads * head_dim
    kv_rows = local_kv * head_dim
    pool_cols = wpool.shape[1]
    channels = pool_cols // 4
    rows = act.shape[0]
    blocks = rows // WINDOW
    chunks = rows // CHUNK
    per_chunk = CHUNK // WINDOW
    half_rows = rows // 2
    half_blocks = blocks // 2
    tiles = width // COLS
    left_tiles = landing_left.shape[0]
    group = heads // local_kv

    def either(for_zero, for_one):
        return for_zero + me_tp * (for_one - for_zero)

    for index in range(n_sp):
        totals[index] = jnp.zeros((8, channels), F32)
    barrier = pltpu.get_barrier_semaphore()

    @pl.when(me_tp == 1)
    def _():
        pl.semaphore_signal(barrier, inc=1, device_id={"tp": 0}, device_id_type=MESH)

    def local_tokens(c):
        return pltpu.make_async_copy(
            tokens.at[pl.ds(c * CHUNK, CHUNK), :], tok.at[c, me_tp], tok_sem.at[c]
        )

    def token_copy(source, where, index):
        return pltpu.make_async_remote_copy(
            src_ref=source,
            dst_ref=where,
            send_sem=tok_send.at[index],
            recv_sem=tok_recv.at[index],
            device_id={"tp": other},
            device_id_type=MESH,
        )

    def remote_tokens(c):
        return token_copy(tok.at[c, me_tp], tok.at[c, me_tp], c)

    lead = chunks - 1
    piece = CHUNK // LEAD_PARTS

    def remote_lead(k):
        return token_copy(
            tokens.at[pl.ds(lead * CHUNK + k * piece, piece), :],
            tok.at[lead, me_tp, pl.ds(k * piece, piece), :],
            lead + k,
        )

    load_wp = pltpu.make_async_copy(wp, wp_raw, w_sem.at[0])
    load_gain = pltpu.make_async_copy(gain_hbm, gain, w_sem.at[1])
    loads = [
        pltpu.make_async_copy(wq, wqkv.at[pl.ds(0, q_rows), :], w_sem.at[2]),
        pltpu.make_async_copy(wk, wqkv.at[pl.ds(q_rows, kv_rows), :], w_sem.at[3]),
        pltpu.make_async_copy(wv, wqkv.at[pl.ds(q_rows + kv_rows, kv_rows), :], w_sem.at[4]),
    ]
    load_out = [
        pltpu.make_async_copy(wo, wout.at[pl.ds(0, q_rows), :], w_sem.at[5]),
        pltpu.make_async_copy(wpo, wout.at[pl.ds(q_rows, 4 * channels), :], w_sem.at[6]),
    ]
    load_sink = pltpu.make_async_copy(sink_hbm, sink, w_sem.at[7])
    for c in reversed(range(chunks)):
        local_tokens(c).start()
    load_gain.start()
    for load in loads + [load_wp] + load_out:
        load.start(priority=1)
    load_sink.start()

    with scope("barrier"):

        @pl.when(me_tp == 0)
        def _():
            pl.semaphore_wait(barrier, 1)
            pl.semaphore_signal(ready.at[0], inc=1, device_id={"tp": 1}, device_id_type=MESH)

        @pl.when(me_tp == 1)
        def _():
            pl.semaphore_wait(ready.at[0], 1)

    for k in range(LEAD_PARTS):
        remote_lead(k).start()
    for step in range(1, n_sp):

        @pl.when((me_tp == 1) & (me_sp - step >= 0))
        def _():
            pl.semaphore_signal(
                barrier,
                inc=1,
                device_id={"sp": lax.rem(me_sp - step + n_sp, n_sp)},
                device_id_type=MESH,
            )

    target = lax.broadcasted_iota(jnp.int32, (WINDOW, 2 * WINDOW), 0) + WINDOW
    source = lax.broadcasted_iota(jnp.int32, (WINDOW, 2 * WINDOW), 1)
    gap = target - source
    for g, reach in enumerate(REACHES):
        bands[g] = jnp.where((gap >= 0) & (gap < reach), 1.0, 0.0).astype(BF16)
    bands[3] = jnp.where((gap >= 0) & (gap < WINDOW) & (source >= WINDOW), 1.0, 0.0).astype(BF16)
    own_key = lax.broadcasted_iota(jnp.int32, (WINDOW, PAIR * WINDOW), 0) <= lax.rem(
        lax.broadcasted_iota(jnp.int32, (WINDOW, PAIR * WINDOW), 1), jnp.int32(WINDOW)
    )
    tri[...] = jnp.where(own_key, 1.0, 0.0).astype(BF16)
    ext[pl.ds(0, WINDOW - TAIL), :] = jnp.zeros((WINDOW - TAIL, pool_cols), BF16)

    @pl.when(me_sp == 0)
    def _():
        ext[pl.ds(WINDOW - TAIL, TAIL), :] = jnp.zeros((TAIL, pool_cols), BF16)
        keys[0] = jnp.zeros((WINDOW, kv_rows), BF16)
        vals[0] = jnp.zeros((kv_rows, WINDOW), BF16)

    def halo_copy(src, dst, index):
        return pltpu.make_async_remote_copy(
            src_ref=src,
            dst_ref=dst,
            send_sem=halo_send.at[index],
            recv_sem=halo_recv.at[index],
            device_id={"sp": lax.rem(me_sp + 1, n_sp)},
            device_id_type=MESH,
        )

    halos = [
        halo_copy(keys.at[blocks], keys.at[0], 0),
        halo_copy(vals.at[blocks], vals.at[0], 1),
        halo_copy(
            ext.at[pl.ds(WINDOW + rows - TAIL, TAIL), :],
            ext.at[pl.ds(WINDOW - TAIL, TAIL), :],
            2,
        ),
    ]

    def total_copy(step):
        return pltpu.make_async_remote_copy(
            src_ref=totals.at[me_sp],
            dst_ref=totals.at[me_sp],
            send_sem=tot_send.at[step],
            recv_sem=tot_recv.at[step],
            device_id={"sp": lax.rem(me_sp + step, n_sp)},
            device_id_type=MESH,
        )

    scale = head_dim ** (-0.5)

    def qkv(c, source):
        half = wqkv.shape[0] // 2
        low = dot(wqkv[pl.ds(0, half), :], source, ((1,), (1,)))
        high = dot(wqkv[pl.ds(half, half), :], source, ((1,), (1,)))
        split = q_rows - half
        for j in range(per_chunk):
            b = c * per_chunk + j
            at = slice(j * WINDOW, (j + 1) * WINDOW)
            qt[b, pl.ds(0, half), :] = (low[:, at] * scale).astype(BF16)
            qt[b, pl.ds(half, split), :] = (high[:split, at] * scale).astype(BF16)
            keys[b + 1] = high[split : split + kv_rows, at].T.astype(BF16)
            vals[b + 1] = high[split + kv_rows :, at].astype(BF16)

    def ext_chunk(c):
        return ext.at[pl.ds(WINDOW + c * CHUNK, CHUNK), :]

    none = jnp.zeros((head_dim, PAIR * WINDOW), BF16)

    def unit_scores(unit):
        b, h, p, edge = unit
        first_head = h * group + p * PAIR
        q = jnp.concatenate(
            [qt[b, pl.ds((first_head + g) * head_dim, head_dim), :] for g in range(PAIR)],
            axis=1,
        )
        rhs = jnp.concatenate([q if k == h else none for k in range(local_kv)], axis=0)
        return dot(keys[b], rhs), dot(keys[b + 1], rhs)

    def unit_weights(unit, scores):
        b, h, p, edge = unit
        first_head = h * group + p * PAIR
        before, own = scores
        if edge:
            before = before + jnp.where((b == 0) & (me_sp == 0), -jnp.inf, 0.0).astype(F32)
        s = jnp.concatenate(
            [jnp.full((1, WINDOW), sink[first_head + g], F32) for g in range(PAIR)], axis=1
        )
        score = jnp.where(own_key, own, before)
        top = jnp.maximum(jnp.max(score, axis=0, keepdims=True), s)
        expo = jnp.exp(score - top)
        total = jnp.sum(expo, axis=0, keepdims=True) + jnp.exp(s - top)
        weight = (expo * (1.0 / total)).astype(BF16)
        w_own = weight * tri[...]
        return jnp.concatenate([weight - w_own, w_own], axis=0)

    def block_rows(b):
        return pl.ds(pl.multiple_of(b * WINDOW, WINDOW), WINDOW)

    def unit_output(unit, weights):
        b, h, p, edge = unit
        first_head = h * group + p * PAIR
        v_at = pl.ds(h * head_dim, head_dim)
        v = jnp.concatenate([vals[b, v_at, :], vals[b + 1, v_at, :]], axis=1)
        gathered = dot(v, weights)
        stacked = jnp.concatenate(
            [gathered[:, g * WINDOW : (g + 1) * WINDOW] for g in range(PAIR)], axis=0
        )
        act[block_rows(b), pl.ds(first_head * head_dim, PAIR * head_dim)] = stacked.T.astype(BF16)

    ascending = [blocks - 1, 1, 0] + list(range(2, blocks - 1))
    sequence = [either(blocks - 1 - i, ascending[i]) for i in range(blocks)]
    units = [
        (sequence[i], h, p, 0 in (blocks - 1 - i, ascending[i]))
        for i in range(blocks)
        for h in range(local_kv)
        for p in range(group // PAIR)
    ]
    per_block = len(units) // blocks
    scores, weights = {}, {}

    def score(first, count):
        for u in range(first, first + count):
            scores[u] = unit_scores(units[u])

    def soften(first, count):
        for u in range(first, first + count):
            weights[u] = unit_weights(units[u], scores.pop(u))

    def gather(first, count):
        for u in range(first, first + count):
            unit_output(units[u], weights.pop(u))

    def pool(b, groups, carried=None):
        start = pl.multiple_of(b * WINDOW, WINDOW)
        position = me_sp * rows + b * WINDOW + 1
        count = (lax.broadcasted_iota(jnp.int32, (WINDOW, channels), 0) + position).astype(F32)
        for g in groups:
            col = pl.ds(g * channels, channels)
            own = ext[pl.ds(start + WINDOW, WINDOW), col]
            if g < 3:
                sums = dot(bands[g], ext[pl.ds(start, 2 * WINDOW), col])
                denom = jnp.minimum(count, float(REACHES[g]))
            else:
                base = carried
                for earlier in range(blocks):
                    base = base + jnp.where(earlier < b, block_sum[earlier], 0.0)
                sums = dot(bands[3, :, pl.ds(WINDOW, WINDOW)], own) + base[:1]
                denom = count
            pooled = sums * (1.0 / denom) - own.astype(F32)
            act[block_rows(b), pl.ds(q_rows + g * channels, channels)] = pooled.astype(BF16)

    def columns(t):
        return pl.ds(t * COLS, COLS)

    def partial_send(t):
        left = t < left_tiles
        return pltpu.make_async_remote_copy(
            src_ref=sending.at[t],
            dst_ref=landing_left.at[t] if left else landing_right.at[t - left_tiles],
            send_sem=out_send.at[t],
            recv_sem=out_recv.at[t],
            device_id={"tp": other},
            device_id_type=MESH,
        )

    with scope("send_tokens"):
        for c in reversed(range(chunks - 1)):
            local_tokens(c).wait()
            remote_tokens(c).start()
    part = 4 * CHUNK

    def regroup(i):
        rows_at = pl.ds(i * part, part)
        wp_f32[rows_at, :] = wp_raw[rows_at, :].astype(F32)
        for g in range(4):
            wpool[pl.ds(i * CHUNK, CHUNK), pl.ds(g * channels, channels)] = wp_f32[
                pl.ds(i * part + g, CHUNK, stride=4), :
            ].astype(BF16)

    def normalize_chunk(c):
        normalize(tok.at[c, 0], tok.at[c, 1], gain, store_into(normed.at[c]))

    with scope("wait_tokens"):
        load_gain.wait()
        local_tokens(lead).wait()
    for k in range(LEAD_PARTS):
        with scope("wait_tokens"):
            remote_lead(k).wait_recv()
        with scope("normalize"):
            at = pl.ds(k * piece, piece)
            normalize(
                tok.at[lead, 0, at, :],
                tok.at[lead, 1, at, :],
                gain,
                store_into(normed.at[lead, at, :]),
            )
    def pool_chunk(c):
        project_pool(
            normed.at[c], wpool, ext_chunk(c), block_sum.at[pl.ds(c * per_chunk, per_chunk)]
        )

    with scope("wait_wqkv"):
        for load in loads:
            load.wait()
    with scope("lead_qkv"):
        qkv(lead, normed[lead])
    with scope("wait_wp"):
        load_wp.wait()
        remote_tokens(chunks - 2).wait_recv()
    with scope("first"):
        for i in range(wp_raw.shape[0] // part):
            regroup(i)
        normalize_chunk(chunks - 2)
        pool_chunk(chunks - 1)
    with scope("sp_ready"):

        @pl.when(me_sp < n_sp - 1)
        def _():
            @pl.when(me_tp == 1)
            def _():
                pl.semaphore_wait(barrier, n_sp - 1 - me_sp)
                pl.semaphore_signal(ready.at[1], inc=1, device_id={"tp": 0}, device_id_type=MESH)

            @pl.when(me_tp == 0)
            def _():
                pl.semaphore_wait(ready.at[1], 1)

    @pl.when(me_sp < n_sp - 1)
    def _():
        for halo in halos:
            halo.start()

    with scope("wait_tokens"):
        for c in reversed(range(chunks - 2)):
            remote_tokens(c).wait_recv()
    with scope("pool_proj"):
        for c in reversed(range(chunks - 1)):
            pool_chunk(c)
            if c > 0:
                normalize_chunk(c - 1)
        all_rows = block_sum[0]
        for b in range(1, blocks):
            all_rows = all_rows + block_sum[b]
        totals[me_sp] = all_rows

    for step in range(1, n_sp):

        @pl.when(me_sp + step < n_sp)
        def _():
            total_copy(step).start()

    load_sink.wait()
    give_first = other * half_blocks
    keep_first = me_tp * half_blocks

    def half_of(first):
        return act[pl.ds(pl.multiple_of(first * WINDOW, WINDOW), half_rows), :]

    def give(t):
        sending[t] = dot(half_of(give_first), wout[:, columns(t)]).astype(BF16)

    def wait_halo(tp):
        with scope("wait_halo"):

            @pl.when((me_sp > 0) & (me_tp == tp))
            def _():
                for halo in halos:
                    halo.wait_recv()

    first = 0
    for i in range(1, chunks):
        c = either(chunks - 1 - i, i - 1)
        count = per_block * i
        if i == chunks - 1:
            wait_halo(1)
        with scope("qkv_rest"):
            score(first, count)
            soften(first, count)
            qkv(c, normed[c])
            gather(first, count)
        first += count

    with scope("attend_a"):
        score(first, per_block)
        soften(first, per_block)
        for i in range(half_blocks):
            for g in range(3):
                pool(give_first + i, (g,))
        gather(first, per_block)
    first += per_block
    with scope("wait_totals"):
        for step in range(1, n_sp):

            @pl.when(me_sp - step >= 0)
            def _():
                total_copy(step).wait_recv()

    carried = jnp.zeros((8, channels), F32)
    for index in range(n_sp):
        carried = carried + jnp.where(index < me_sp, totals[index], 0.0)
    left = len(units) - first
    with scope("pool_b"):
        score(first, left // tiles)
        for i in range(half_blocks):
            pool(give_first + i, (3,), carried)

    keep_pieces = [(i, g) for i in reversed(range(half_blocks)) for g in range(4)]
    for load in load_out:
        load.wait()
    for t in range(tiles):
        if t == 1:
            wait_halo(0)
        with scope("give"):
            lo, hi = first + t * left // tiles, first + (t + 1) * left // tiles
            soften(lo, hi - lo)
            give(t)
            gather(lo, hi - lo)
            if t < tiles - 1:
                score(hi, first + (t + 2) * left // tiles - hi)
            at = [len(keep_pieces) * k // tiles for k in (t, t + 1)]
            for i, g in keep_pieces[at[0] : at[1]]:
                pool(keep_first + i, (g,), carried)
        partial_send(t).start()
    for group_tiles in (range(left_tiles - 1), range(left_tiles - 1, left_tiles)):
        with scope("wait_give"):
            for t in group_tiles:
                partial_send(t).wait_recv()
        with scope("keep"):
            for t in group_tiles:
                mine = dot(half_of(keep_first), wout[:, columns(t)])
                out_left[:, columns(t)] = (mine + landing_left[t].astype(F32)).astype(BF16)
    with scope("end_mix"):
        for t in range(left_tiles, tiles):
            partial_send(t).wait_recv()
        for t in range(tiles):
            partial_send(t).wait_send()
        for c in range(lead):
            remote_tokens(c).wait_send()
        for k in range(LEAD_PARTS):
            remote_lead(k).wait_send()
        for step in range(1, n_sp):

            @pl.when(me_sp + step < n_sp)
            def _():
                total_copy(step).wait_send()

        @pl.when(me_sp < n_sp - 1)
        def _():
            for halo in halos:
                halo.wait_send()


def finish_kernel(act, wout, out_left, landing_right, out, out_right, sem):
    me_tp = lax.axis_index("tp")
    half_rows, left_width = out_left.shape
    right_tiles = landing_right.shape[0]
    left = pltpu.make_async_copy(out_left, out.at[:, pl.ds(0, left_width)], sem.at[0])
    left.start()

    def right(t):
        at = pl.ds(left_width + t * COLS, COLS)
        return pltpu.make_async_copy(out_right.at[t], out.at[:, at], sem.at[1 + t])

    mine = act[pl.ds(pl.multiple_of(me_tp * half_rows, half_rows), half_rows), :]
    for t in range(right_tiles):
        at = pl.ds(left_width + t * COLS, COLS)
        out_right[t] = (dot(mine, wout[:, at]) + landing_right[t].astype(F32)).astype(BF16)
        right(t).start()
    left.wait()
    for t in range(right_tiles):
        right(t).wait()


def shards(n_sp, tokens, gain, wq, wk, wv, sink, wp, wo, wpo):
    rows, half_width = tokens.shape[1:]
    width = 2 * half_width
    heads, head_dim = wq.shape[1:]
    local_kv = wk.shape[1]
    channels = wp.shape[2]
    q_rows, kv_rows = (heads * head_dim, local_kv * head_dim)
    pool_cols = 4 * channels
    blocks = rows // WINDOW
    tiles = width // COLS
    left_tiles = tiles - 1
    chunks = rows // CHUNK
    per_chunk = CHUNK // WINDOW
    half_rows = rows // 2
    dma = pltpu.SemaphoreType.DMA
    flat = lambda w: jnp.transpose(w, (1, 2, 0)).reshape(-1, width)
    hbm = pl.BlockSpec(memory_space=pltpu.HBM)
    vmem = pl.BlockSpec(memory_space=pltpu.VMEM)

    mixed = [
        ((rows, q_rows + pool_cols), BF16),
        ((half_rows, left_tiles * COLS), BF16),
        ((tiles - left_tiles, half_rows, COLS), BF16),
        ((q_rows + pool_cols, width), BF16),
    ]
    size = lambda shapes: sum(
        functools.reduce(lambda a, b: a * b, s) * jnp.dtype(d).itemsize for s, d in shapes
    )
    spare = 67043328 - 262144
    act, out_left, landing_right, wout = pl.pallas_call(
        functools.partial(mix_kernel, n_sp, heads, local_kv, head_dim),
        out_shape=[pltpu.VMEM(s, d) for s, d in mixed],
        in_specs=[hbm] * 9,
        out_specs=[vmem] * len(mixed),
        scratch_shapes=[
            pltpu.VMEM((chunks, 2, CHUNK, half_width), BF16),
            pltpu.VMEM((chunks, CHUNK, width), BF16),
            pltpu.VMEM((1, width), F32),
            pltpu.SMEM((heads,), F32),
            pltpu.VMEM((4 * width, channels), BF16),
            pltpu.VMEM((4 * width, channels), F32),
            pltpu.VMEM((width, pool_cols), BF16),
            pltpu.VMEM((q_rows + 2 * kv_rows, width), BF16),
            pltpu.VMEM((WINDOW, PAIR * WINDOW), BF16),
            pltpu.VMEM((4, WINDOW, 2 * WINDOW), BF16),
            pltpu.VMEM((blocks, q_rows, WINDOW), BF16),
            pltpu.VMEM((blocks + 1, WINDOW, kv_rows), BF16),
            pltpu.VMEM((blocks + 1, kv_rows, WINDOW), BF16),
            pltpu.VMEM((rows + WINDOW, pool_cols), BF16),
            pltpu.VMEM((blocks, 8, channels), F32),
            pltpu.VMEM((n_sp, 8, channels), F32),
            pltpu.VMEM((tiles, half_rows, COLS), BF16),
            pltpu.VMEM((left_tiles, half_rows, COLS), BF16),
            dma((8,)),
            dma((chunks,)),
            dma((chunks - 1 + LEAD_PARTS,)),
            dma((chunks - 1 + LEAD_PARTS,)),
            dma((3,)),
            dma((3,)),
            dma((n_sp,)),
            dma((n_sp,)),
            dma((tiles,)),
            dma((tiles,)),
            pltpu.SemaphoreType.REGULAR((2,)),
        ],
        compiler_params=pltpu.CompilerParams(
            collective_id=0, has_side_effects=True, vmem_limit_bytes=spare - size(mixed)
        ),
    )(
        tokens[0],
        gain.reshape(1, width),
        flat(wq),
        flat(wk),
        flat(wv),
        wp.reshape(-1, channels),
        wo.reshape(-1, width),
        wpo.reshape(-1, width),
        sink,
    )
    result = pl.pallas_call(
        finish_kernel,
        out_shape=jax.ShapeDtypeStruct((half_rows, width), BF16),
        in_specs=[vmem] * 4,
        out_specs=hbm,
        scratch_shapes=[
            pltpu.VMEM((tiles - left_tiles, half_rows, COLS), BF16),
            dma((1 + tiles - left_tiles,)),
        ],
        compiler_params=pltpu.CompilerParams(vmem_limit_bytes=spare // 3),
    )(act, wout, out_left, landing_right)
    return result[None]


def solution(mesh):
    in_specs = (
        P("fs", ("grp", "sp"), "tp"),
        P(),
        P(None, "tp", None),
        P(None, "tp", None),
        P(None, "tp", None),
        P("tp"),
        P(None, None, "tp"),
        P("tp", None, None),
        P(None, "tp", None),
    )
    out_specs = P("fs", ("grp", "sp", "tp"), None)
    return jax.shard_map(
        functools.partial(shards, mesh.shape["sp"]),
        mesh=mesh,
        in_specs=in_specs,
        out_specs=out_specs,
        check_vma=False,
    )
```

```python
import functools

import jax
import jax.numpy as jnp
from jax import lax
from jax.experimental import pallas as pl
from jax.experimental.pallas import tpu as pltpu
from jax.sharding import PartitionSpec as P

MESH = pl.DeviceIdType.MESH
WINDOW = 128
REACHES = (2, 4, 16)
TAIL = 16
CHUNK = 256
COLS = 512
PAIR = 2
LEAD_PARTS = 4
FINAL_PARTS = 2
F32 = jnp.float32
BF16 = jnp.bfloat16
scope = jax.named_scope


def dot(a, b, dims=((1,), (0,))):
    return lax.dot_general(a, b, (dims, ((), ())), preferred_element_type=F32)


def normalize(low_ref, high_ref, gain, store):
    half_width = low_ref.shape[1]
    low = low_ref[...].astype(F32)
    high = high_ref[...].astype(F32)
    square = jnp.sum(low * low, axis=1, keepdims=True)
    square = square + jnp.sum(high * high, axis=1, keepdims=True)
    inv = lax.rsqrt(square * (0.5 / half_width) + 1e-06)
    low_at, high_at = pl.ds(0, half_width), pl.ds(half_width, half_width)
    store(low_at, (low * inv * gain[:, low_at]).astype(BF16))
    store(high_at, (high * inv * gain[:, high_at]).astype(BF16))


def store_into(ref):
    def store(at, value):
        ref[:, at] = value

    return store


def project_pool(normed, wpool, ext_rows, sums):
    pooled_in = dot(normed[...], wpool[...]).astype(BF16)
    ext_rows[...] = pooled_in
    channels = pooled_in.shape[1] // 4
    last = pooled_in[:, 3 * channels :].astype(F32)
    for j in range(pooled_in.shape[0] // WINDOW):
        summed = jnp.sum(last[j * WINDOW : (j + 1) * WINDOW], axis=0, keepdims=True)
        sums[j] = jnp.broadcast_to(summed, (8, channels))


def mix_kernel(
    n_sp,
    heads,
    local_kv,
    head_dim,
    tokens,
    gain_hbm,
    wq,
    wk,
    wv,
    wp,
    wo,
    wpo,
    sink_hbm,
    act,
    out_left,
    landing_right,
    wout,
    tok,
    normed,
    gain,
    sink,
    wp_raw,
    wp_f32,
    wpool,
    wqkv,
    tri,
    bands,
    qt,
    keys,
    vals,
    ext,
    block_sum,
    totals,
    sending,
    landing_left,
    w_sem,
    tok_sem,
    tok_send,
    tok_recv,
    halo_send,
    halo_recv,
    tot_send,
    tot_recv,
    out_send,
    out_recv,
    ready,
):
    me_sp = lax.axis_index("sp")
    me_tp = lax.axis_index("tp")
    other = 1 - me_tp
    width = wout.shape[1]
    q_rows = heads * head_dim
    kv_rows = local_kv * head_dim
    pool_cols = wpool.shape[1]
    channels = pool_cols // 4
    rows = act.shape[0]
    blocks = rows // WINDOW
    chunks = rows // CHUNK
    per_chunk = CHUNK // WINDOW
    half_rows = rows // 2
    half_blocks = blocks // 2
    tiles = width // COLS
    left_tiles = landing_left.shape[0]
    group = heads // local_kv

    def either(for_zero, for_one):
        return for_zero + me_tp * (for_one - for_zero)

    for index in range(n_sp):
        totals[index] = jnp.zeros((8, channels), F32)
    barrier = pltpu.get_barrier_semaphore()

    @pl.when(me_tp == 1)
    def _():
        pl.semaphore_signal(barrier, inc=1, device_id={"tp": 0}, device_id_type=MESH)

    def local_tokens(c):
        return pltpu.make_async_copy(
            tokens.at[pl.ds(c * CHUNK, CHUNK), :], tok.at[c, me_tp], tok_sem.at[c]
        )

    def token_copy(source, where, index):
        return pltpu.make_async_remote_copy(
            src_ref=source,
            dst_ref=where,
            send_sem=tok_send.at[index],
            recv_sem=tok_recv.at[index],
            device_id={"tp": other},
            device_id_type=MESH,
        )

    def remote_tokens(c):
        return token_copy(tok.at[c, me_tp], tok.at[c, me_tp], c)

    lead = chunks - 1
    piece = CHUNK // LEAD_PARTS

    def remote_lead(k):
        return token_copy(
            tokens.at[pl.ds(lead * CHUNK + k * piece, piece), :],
            tok.at[lead, me_tp, pl.ds(k * piece, piece), :],
            lead + k,
        )

    load_wp = pltpu.make_async_copy(wp, wp_raw, w_sem.at[0])
    load_gain = pltpu.make_async_copy(gain_hbm, gain, w_sem.at[1])
    loads = [
        pltpu.make_async_copy(wq, wqkv.at[pl.ds(0, q_rows), :], w_sem.at[2]),
        pltpu.make_async_copy(wk, wqkv.at[pl.ds(q_rows, kv_rows), :], w_sem.at[3]),
        pltpu.make_async_copy(wv, wqkv.at[pl.ds(q_rows + kv_rows, kv_rows), :], w_sem.at[4]),
    ]
    load_out = [
        pltpu.make_async_copy(wo, wout.at[pl.ds(0, q_rows), :], w_sem.at[5]),
        pltpu.make_async_copy(wpo, wout.at[pl.ds(q_rows, 4 * channels), :], w_sem.at[6]),
    ]
    load_sink = pltpu.make_async_copy(sink_hbm, sink, w_sem.at[7])
    for c in reversed(range(chunks)):
        local_tokens(c).start()
    load_gain.start()
    for load in loads + [load_wp] + load_out:
        load.start(priority=1)
    load_sink.start()

    with scope("barrier"):

        @pl.when(me_tp == 0)
        def _():
            pl.semaphore_wait(barrier, 1)
            pl.semaphore_signal(ready.at[0], inc=1, device_id={"tp": 1}, device_id_type=MESH)

        @pl.when(me_tp == 1)
        def _():
            pl.semaphore_wait(ready.at[0], 1)

    for k in range(LEAD_PARTS):
        remote_lead(k).start()
    for step in range(1, n_sp):

        @pl.when((me_tp == 1) & (me_sp - step >= 0))
        def _():
            pl.semaphore_signal(
                barrier,
                inc=1,
                device_id={"sp": lax.rem(me_sp - step + n_sp, n_sp)},
                device_id_type=MESH,
            )

    target = lax.broadcasted_iota(jnp.int32, (WINDOW, 2 * WINDOW), 0) + WINDOW
    source = lax.broadcasted_iota(jnp.int32, (WINDOW, 2 * WINDOW), 1)
    gap = target - source
    for g, reach in enumerate(REACHES):
        bands[g] = jnp.where((gap >= 0) & (gap < reach), 1.0, 0.0).astype(BF16)
    bands[3] = jnp.where((gap >= 0) & (gap < WINDOW) & (source >= WINDOW), 1.0, 0.0).astype(BF16)
    own_key = lax.broadcasted_iota(jnp.int32, (WINDOW, PAIR * WINDOW), 0) <= lax.rem(
        lax.broadcasted_iota(jnp.int32, (WINDOW, PAIR * WINDOW), 1), jnp.int32(WINDOW)
    )
    tri[...] = jnp.where(own_key, 1.0, 0.0).astype(BF16)
    ext[pl.ds(0, WINDOW - TAIL), :] = jnp.zeros((WINDOW - TAIL, pool_cols), BF16)

    @pl.when(me_sp == 0)
    def _():
        ext[pl.ds(WINDOW - TAIL, TAIL), :] = jnp.zeros((TAIL, pool_cols), BF16)
        keys[0] = jnp.zeros((WINDOW, kv_rows), BF16)
        vals[0] = jnp.zeros((kv_rows, WINDOW), BF16)

    def halo_copy(src, dst, index):
        return pltpu.make_async_remote_copy(
            src_ref=src,
            dst_ref=dst,
            send_sem=halo_send.at[index],
            recv_sem=halo_recv.at[index],
            device_id={"sp": lax.rem(me_sp + 1, n_sp)},
            device_id_type=MESH,
        )

    halos = [
        halo_copy(keys.at[blocks], keys.at[0], 0),
        halo_copy(vals.at[blocks], vals.at[0], 1),
        halo_copy(
            ext.at[pl.ds(WINDOW + rows - TAIL, TAIL), :],
            ext.at[pl.ds(WINDOW - TAIL, TAIL), :],
            2,
        ),
    ]

    def total_copy(step):
        return pltpu.make_async_remote_copy(
            src_ref=totals.at[me_sp],
            dst_ref=totals.at[me_sp],
            send_sem=tot_send.at[step],
            recv_sem=tot_recv.at[step],
            device_id={"sp": lax.rem(me_sp + step, n_sp)},
            device_id_type=MESH,
        )

    scale = head_dim ** (-0.5)

    def qkv(c, source):
        half = wqkv.shape[0] // 2
        low = dot(wqkv[pl.ds(0, half), :], source, ((1,), (1,)))
        high = dot(wqkv[pl.ds(half, half), :], source, ((1,), (1,)))
        split = q_rows - half
        for j in range(per_chunk):
            b = c * per_chunk + j
            at = slice(j * WINDOW, (j + 1) * WINDOW)
            qt[b, pl.ds(0, half), :] = (low[:, at] * scale).astype(BF16)
            qt[b, pl.ds(half, split), :] = (high[:split, at] * scale).astype(BF16)
            keys[b + 1] = high[split : split + kv_rows, at].T.astype(BF16)
            vals[b + 1] = high[split + kv_rows :, at].astype(BF16)

    def ext_chunk(c):
        return ext.at[pl.ds(WINDOW + c * CHUNK, CHUNK), :]

    none = jnp.zeros((head_dim, PAIR * WINDOW), BF16)

    def unit_scores(unit):
        b, h, p, edge = unit
        first_head = h * group + p * PAIR
        q = jnp.concatenate(
            [qt[b, pl.ds((first_head + g) * head_dim, head_dim), :] for g in range(PAIR)],
            axis=1,
        )
        rhs = jnp.concatenate([q if k == h else none for k in range(local_kv)], axis=0)
        return dot(keys[b], rhs), dot(keys[b + 1], rhs)

    def unit_weights(unit, scores):
        b, h, p, edge = unit
        first_head = h * group + p * PAIR
        before, own = scores
        if edge:
            before = before + jnp.where((b == 0) & (me_sp == 0), -jnp.inf, 0.0).astype(F32)
        s = jnp.concatenate(
            [jnp.full((1, WINDOW), sink[first_head + g], F32) for g in range(PAIR)], axis=1
        )
        score = jnp.where(own_key, own, before)
        top = jnp.maximum(jnp.max(score, axis=0, keepdims=True), s)
        expo = jnp.exp(score - top)
        total = jnp.sum(expo, axis=0, keepdims=True) + jnp.exp(s - top)
        weight = (expo * (1.0 / total)).astype(BF16)
        w_own = weight * tri[...]
        return jnp.concatenate([weight - w_own, w_own], axis=0)

    def block_rows(b):
        return pl.ds(pl.multiple_of(b * WINDOW, WINDOW), WINDOW)

    def unit_output(unit, weights):
        b, h, p, edge = unit
        first_head = h * group + p * PAIR
        v_at = pl.ds(h * head_dim, head_dim)
        v = jnp.concatenate([vals[b, v_at, :], vals[b + 1, v_at, :]], axis=1)
        gathered = dot(v, weights)
        stacked = jnp.concatenate(
            [gathered[:, g * WINDOW : (g + 1) * WINDOW] for g in range(PAIR)], axis=0
        )
        act[block_rows(b), pl.ds(first_head * head_dim, PAIR * head_dim)] = stacked.T.astype(BF16)

    ascending = [blocks - 1, 1, 0] + list(range(2, blocks - 1))
    sequence = [either(blocks - 1 - i, ascending[i]) for i in range(blocks)]
    units = [
        (sequence[i], h, p, 0 in (blocks - 1 - i, ascending[i]))
        for i in range(blocks)
        for h in range(local_kv)
        for p in range(group // PAIR)
    ]
    per_block = len(units) // blocks
    scores, weights = {}, {}

    def score(first, count):
        for u in range(first, first + count):
            scores[u] = unit_scores(units[u])

    def soften(first, count):
        for u in range(first, first + count):
            weights[u] = unit_weights(units[u], scores.pop(u))

    def gather(first, count):
        for u in range(first, first + count):
            unit_output(units[u], weights.pop(u))

    def pool(b, groups, carried=None):
        start = pl.multiple_of(b * WINDOW, WINDOW)
        position = me_sp * rows + b * WINDOW + 1
        count = (lax.broadcasted_iota(jnp.int32, (WINDOW, channels), 0) + position).astype(F32)
        for g in groups:
            col = pl.ds(g * channels, channels)
            own = ext[pl.ds(start + WINDOW, WINDOW), col]
            if g < 3:
                sums = dot(bands[g], ext[pl.ds(start, 2 * WINDOW), col])
                denom = jnp.minimum(count, float(REACHES[g]))
            else:
                base = carried
                for earlier in range(blocks):
                    base = base + jnp.where(earlier < b, block_sum[earlier], 0.0)
                sums = dot(bands[3, :, pl.ds(WINDOW, WINDOW)], own) + base[:1]
                denom = count
            pooled = sums * (1.0 / denom) - own.astype(F32)
            act[block_rows(b), pl.ds(q_rows + g * channels, channels)] = pooled.astype(BF16)

    def columns(t):
        return pl.ds(t * COLS, COLS)

    def partial_send(t):
        left = t < left_tiles
        return pltpu.make_async_remote_copy(
            src_ref=sending.at[t],
            dst_ref=landing_left.at[t] if left else landing_right.at[t - left_tiles],
            send_sem=out_send.at[t],
            recv_sem=out_recv.at[t],
            device_id={"tp": other},
            device_id_type=MESH,
        )

    with scope("send_tokens"):
        for c in reversed(range(chunks - 1)):
            local_tokens(c).wait()
            remote_tokens(c).start()
    part = 4 * CHUNK

    def regroup(i):
        rows_at = pl.ds(i * part, part)
        wp_f32[rows_at, :] = wp_raw[rows_at, :].astype(F32)
        for g in range(4):
            wpool[pl.ds(i * CHUNK, CHUNK), pl.ds(g * channels, channels)] = wp_f32[
                pl.ds(i * part + g, CHUNK, stride=4), :
            ].astype(BF16)

    def normalize_chunk(c):
        normalize(tok.at[c, 0], tok.at[c, 1], gain, store_into(normed.at[c]))

    with scope("wait_tokens"):
        load_gain.wait()
        local_tokens(lead).wait()
    for k in range(LEAD_PARTS):
        with scope("wait_tokens"):
            remote_lead(k).wait_recv()
        with scope("normalize"):
            at = pl.ds(k * piece, piece)
            normalize(
                tok.at[lead, 0, at, :],
                tok.at[lead, 1, at, :],
                gain,
                store_into(normed.at[lead, at, :]),
            )
    def pool_chunk(c):
        project_pool(
            normed.at[c], wpool, ext_chunk(c), block_sum.at[pl.ds(c * per_chunk, per_chunk)]
        )

    with scope("wait_wqkv"):
        for load in loads:
            load.wait()
    with scope("lead_qkv"):
        qkv(lead, normed[lead])
    with scope("wait_wp"):
        load_wp.wait()
        remote_tokens(chunks - 2).wait_recv()
    with scope("first"):
        for i in range(wp_raw.shape[0] // part):
            regroup(i)
        normalize_chunk(chunks - 2)
        pool_chunk(chunks - 1)
    with scope("sp_ready"):

        @pl.when(me_sp < n_sp - 1)
        def _():
            @pl.when(me_tp == 1)
            def _():
                pl.semaphore_wait(barrier, n_sp - 1 - me_sp)
                pl.semaphore_signal(ready.at[1], inc=1, device_id={"tp": 0}, device_id_type=MESH)

            @pl.when(me_tp == 0)
            def _():
                pl.semaphore_wait(ready.at[1], 1)

    @pl.when(me_sp < n_sp - 1)
    def _():
        for halo in halos:
            halo.start()

    with scope("wait_tokens"):
        for c in reversed(range(chunks - 2)):
            remote_tokens(c).wait_recv()
    with scope("pool_proj"):
        for c in reversed(range(chunks - 1)):
            pool_chunk(c)
            if c > 0:
                normalize_chunk(c - 1)
        all_rows = block_sum[0]
        for b in range(1, blocks):
            all_rows = all_rows + block_sum[b]
        totals[me_sp] = all_rows

    for step in range(1, n_sp):

        @pl.when(me_sp + step < n_sp)
        def _():
            total_copy(step).start()

    load_sink.wait()
    give_first = other * half_blocks
    keep_first = me_tp * half_blocks

    def half_of(first):
        return act[pl.ds(pl.multiple_of(first * WINDOW, WINDOW), half_rows), :]

    def give(t):
        sending[t] = dot(half_of(give_first), wout[:, columns(t)]).astype(BF16)

    def wait_halo(tp):
        with scope("wait_halo"):

            @pl.when((me_sp > 0) & (me_tp == tp))
            def _():
                for halo in halos:
                    halo.wait_recv()

    first = 0
    for i in range(1, chunks):
        c = either(chunks - 1 - i, i - 1)
        count = per_block * i
        if i == chunks - 1:
            wait_halo(1)
        with scope("qkv_rest"):
            score(first, count)
            soften(first, count)
            qkv(c, normed[c])
            gather(first, count)
        first += count

    with scope("attend_a"):
        score(first, per_block)
        soften(first, per_block)
        for i in range(half_blocks):
            for g in range(3):
                pool(give_first + i, (g,))
        gather(first, per_block)
    first += per_block
    with scope("wait_totals"):
        for step in range(1, n_sp):

            @pl.when(me_sp - step >= 0)
            def _():
                total_copy(step).wait_recv()

    carried = jnp.zeros((8, channels), F32)
    for index in range(n_sp):
        carried = carried + jnp.where(index < me_sp, totals[index], 0.0)
    left = len(units) - first
    with scope("pool_b"):
        score(first, left // tiles)
        for i in range(half_blocks):
            pool(give_first + i, (3,), carried)

    keep_pieces = [(i, g) for i in reversed(range(half_blocks)) for g in range(4)]
    for load in load_out:
        load.wait()
    for t in range(tiles):
        if t == 1:
            wait_halo(0)
        with scope("give"):
            lo, hi = first + t * left // tiles, first + (t + 1) * left // tiles
            soften(lo, hi - lo)
            give(t)
            gather(lo, hi - lo)
            if t < tiles - 1:
                score(hi, first + (t + 2) * left // tiles - hi)
            at = [len(keep_pieces) * k // tiles for k in (t, t + 1)]
            for i, g in keep_pieces[at[0] : at[1]]:
                pool(keep_first + i, (g,), carried)
        partial_send(t).start()
    for group_tiles in (range(left_tiles - 1), range(left_tiles - 1, left_tiles)):
        with scope("wait_give"):
            for t in group_tiles:
                partial_send(t).wait_recv()
        with scope("keep"):
            for t in group_tiles:
                mine = dot(half_of(keep_first), wout[:, columns(t)])
                out_left[:, columns(t)] = (mine + landing_left[t].astype(F32)).astype(BF16)
    with scope("end_mix"):
        for t in range(left_tiles, tiles):
            partial_send(t).wait_recv()
        for t in range(tiles):
            partial_send(t).wait_send()
        for c in range(lead):
            remote_tokens(c).wait_send()
        for k in range(LEAD_PARTS):
            remote_lead(k).wait_send()
        for step in range(1, n_sp):

            @pl.when(me_sp + step < n_sp)
            def _():
                total_copy(step).wait_send()

        @pl.when(me_sp < n_sp - 1)
        def _():
            for halo in halos:
                halo.wait_send()


def finish_kernel(act, wout, out_left, landing_right, out, out_right, sem):
    me_tp = lax.axis_index("tp")
    half_rows, left_width = out_left.shape
    right_tiles = landing_right.shape[0]
    left = pltpu.make_async_copy(out_left, out.at[:, pl.ds(0, left_width)], sem.at[0])
    left.start()

    piece = half_rows // FINAL_PARTS

    def right(t, k):
        rows_at = pl.ds(k * piece, piece)
        at = pl.ds(left_width + t * COLS, COLS)
        return pltpu.make_async_copy(
            out_right.at[t, rows_at, :], out.at[rows_at, at], sem.at[1 + t * FINAL_PARTS + k]
        )

    for t in range(right_tiles):
        at = pl.ds(left_width + t * COLS, COLS)
        for k in range(FINAL_PARTS):
            rows_at = pl.ds(k * piece, piece)
            mine = act[pl.ds(pl.multiple_of(me_tp * half_rows + k * piece, piece), piece), :]
            out_right[t, rows_at, :] = (
                dot(mine, wout[:, at]) + landing_right[t, rows_at, :].astype(F32)
            ).astype(BF16)
            right(t, k).start()
    left.wait()
    for t in range(right_tiles):
        for k in range(FINAL_PARTS):
            right(t, k).wait()


def shards(n_sp, tokens, gain, wq, wk, wv, sink, wp, wo, wpo):
    rows, half_width = tokens.shape[1:]
    width = 2 * half_width
    heads, head_dim = wq.shape[1:]
    local_kv = wk.shape[1]
    channels = wp.shape[2]
    q_rows, kv_rows = (heads * head_dim, local_kv * head_dim)
    pool_cols = 4 * channels
    blocks = rows // WINDOW
    tiles = width // COLS
    left_tiles = tiles - 1
    chunks = rows // CHUNK
    per_chunk = CHUNK // WINDOW
    half_rows = rows // 2
    dma = pltpu.SemaphoreType.DMA
    flat = lambda w: jnp.transpose(w, (1, 2, 0)).reshape(-1, width)
    hbm = pl.BlockSpec(memory_space=pltpu.HBM)
    vmem = pl.BlockSpec(memory_space=pltpu.VMEM)

    mixed = [
        ((rows, q_rows + pool_cols), BF16),
        ((half_rows, left_tiles * COLS), BF16),
        ((tiles - left_tiles, half_rows, COLS), BF16),
        ((q_rows + pool_cols, width), BF16),
    ]
    size = lambda shapes: sum(
        functools.reduce(lambda a, b: a * b, s) * jnp.dtype(d).itemsize for s, d in shapes
    )
    spare = 67043328 - 262144
    act, out_left, landing_right, wout = pl.pallas_call(
        functools.partial(mix_kernel, n_sp, heads, local_kv, head_dim),
        out_shape=[pltpu.VMEM(s, d) for s, d in mixed],
        in_specs=[hbm] * 9,
        out_specs=[vmem] * len(mixed),
        scratch_shapes=[
            pltpu.VMEM((chunks, 2, CHUNK, half_width), BF16),
            pltpu.VMEM((chunks, CHUNK, width), BF16),
            pltpu.VMEM((1, width), F32),
            pltpu.SMEM((heads,), F32),
            pltpu.VMEM((4 * width, channels), BF16),
            pltpu.VMEM((4 * width, channels), F32),
            pltpu.VMEM((width, pool_cols), BF16),
            pltpu.VMEM((q_rows + 2 * kv_rows, width), BF16),
            pltpu.VMEM((WINDOW, PAIR * WINDOW), BF16),
            pltpu.VMEM((4, WINDOW, 2 * WINDOW), BF16),
            pltpu.VMEM((blocks, q_rows, WINDOW), BF16),
            pltpu.VMEM((blocks + 1, WINDOW, kv_rows), BF16),
            pltpu.VMEM((blocks + 1, kv_rows, WINDOW), BF16),
            pltpu.VMEM((rows + WINDOW, pool_cols), BF16),
            pltpu.VMEM((blocks, 8, channels), F32),
            pltpu.VMEM((n_sp, 8, channels), F32),
            pltpu.VMEM((tiles, half_rows, COLS), BF16),
            pltpu.VMEM((left_tiles, half_rows, COLS), BF16),
            dma((8,)),
            dma((chunks,)),
            dma((chunks - 1 + LEAD_PARTS,)),
            dma((chunks - 1 + LEAD_PARTS,)),
            dma((3,)),
            dma((3,)),
            dma((n_sp,)),
            dma((n_sp,)),
            dma((tiles,)),
            dma((tiles,)),
            pltpu.SemaphoreType.REGULAR((2,)),
        ],
        compiler_params=pltpu.CompilerParams(
            collective_id=0, has_side_effects=True, vmem_limit_bytes=spare - size(mixed)
        ),
    )(
        tokens[0],
        gain.reshape(1, width),
        flat(wq),
        flat(wk),
        flat(wv),
        wp.reshape(-1, channels),
        wo.reshape(-1, width),
        wpo.reshape(-1, width),
        sink,
    )
    result = pl.pallas_call(
        finish_kernel,
        out_shape=jax.ShapeDtypeStruct((half_rows, width), BF16),
        in_specs=[vmem] * 4,
        out_specs=hbm,
        scratch_shapes=[
            pltpu.VMEM((tiles - left_tiles, half_rows, COLS), BF16),
            dma((1 + (tiles - left_tiles) * FINAL_PARTS,)),
        ],
        compiler_params=pltpu.CompilerParams(vmem_limit_bytes=spare // 3),
    )(act, wout, out_left, landing_right)
    return result[None]


def solution(mesh):
    in_specs = (
        P("fs", ("grp", "sp"), "tp"),
        P(),
        P(None, "tp", None),
        P(None, "tp", None),
        P(None, "tp", None),
        P("tp"),
        P(None, None, "tp"),
        P("tp", None, None),
        P(None, "tp", None),
    )
    out_specs = P("fs", ("grp", "sp", "tp"), None)
    return jax.shard_map(
        functools.partial(shards, mesh.shape["sp"]),
        mesh=mesh,
        in_specs=in_specs,
        out_specs=out_specs,
        check_vma=False,
    )
```
